128 devices in a mesh: sp: 32 (over z, y, core), tp: 4 (over x).
Axes of the slice: x: 4, y: 4, z: 4, core: 2. Of those that a mesh axis runs over, the one named last changes fastest.
Arguments:
- mixer_value_projection: bfloat16 [24576, 2048], P('sp', 'tp'), may hold values from -6 to 6
- write_vectors_projected: bfloat16 [24576, 256], P('sp', 'tp'), may hold values from -6 to 6
- read_vectors_projected: bfloat16 [24576, 256], P('sp', 'tp'), may hold values from -6 to 6
- output_gate_projected: bfloat16 [24576, 2048], P('sp', 'tp'), may hold values from -6 to 6
- step_size_scores: float32 [24576, 32], P('sp', 'tp'), may hold values from -8 to 8
- position_decay_extra: float32 [24576, 32], P('sp', 'tp'), may hold values from -1 to 0
- step_size_bias: float32 [32], P('tp'), may hold values from -1 to 1
- head_decay_logarithm: float32 [32], P('tp'), may hold values from -14 to -3
- value_filter_taps: bfloat16 [4, 2048], P(None, 'tp'), may hold values from -3 to 3
- write_filter_taps: bfloat16 [4, 256], P(None, 'tp'), may hold values from -3 to 3
- read_filter_taps: bfloat16 [4, 256], P(None, 'tp'), may hold values from -3 to 3
- gated_group_norm_gain: float32 [2048], P('tp'), may hold values from 0.1 to 1.9
- mixer_output_weight: bfloat16 [2048, 2048], P('tp'), may hold values from -0.125 to 0.125
- residual: bfloat16 [24576, 2048], P('sp'), may hold values from -6 to 6
- feedforward_norm_gain: float32 [2048], replicated, may hold values from 0.1 to 1.9
- feedforward_gate_weight: bfloat16 [2048, 5632], P('sp', 'tp'), may hold values from -0.125 to 0.125
- feedforward_value_weight: bfloat16 [2048, 5632], P('sp', 'tp'), may hold values from -0.125 to 0.125
- gate_filter_taps: bfloat16 [3, 5632], P(None, 'tp'), may hold values from -3.5 to 3.5
- single_value_filter_taps: bfloat16 [3, 5632], P(None, 'tp'), may hold values from -3.5 to 3.5
- feedforward_down_weight: bfloat16 [5632, 2048], P('tp', 'sp'), may hold values from -0.078125 to 0.078125
Outputs:
- mixed: bfloat16 [24576, 2048], P(('sp', 'tp'))
The draws below stay inside these ranges and needn't reach their ends.
All inputs are finite; a program needn't handle non-finite values.
Results may differ from the reference program's by a relative error of at most 0.012.
Values may be sent and summed in bfloat16 or wider, within the bound.
No kernel may reach another device: no remote copies, remote signals or barrier semaphores. Data moves between devices by JAX's collectives and lax.ppermute only.
A program may use at most 192 MiB of HBM per device.

```python
import jax
import jax.numpy as jnp
from jax import lax

D = 2048
HEADS = 32
HEAD = 64
GROUPS = 4
STATE = 64
FF = 5632
TOK_DEV = 768
BLOCK = 128
CONV_MIX = 4
CONV_FFN = 3
INNER = 2048
SEQ = 24576


def draw_step_size_scores(key, part):
    first, second = jax.random.split(jax.random.fold_in(key, 11))
    block_total = SEQ // TOK_DEV
    base = jax.random.normal(first, (SEQ, HEADS), jnp.float32)
    shifts = jax.random.uniform(second, (block_total, 1, HEADS), jnp.float32, -1.5, 1.5)
    return (base.reshape(block_total, TOK_DEV, HEADS) + shifts).reshape(SEQ, HEADS)


def draw_head_decay_logarithm(key, part):
    first, second, third = jax.random.split(jax.random.fold_in(key, 12), 3)
    share = 0.5
    slowly = jax.random.uniform(first, (HEADS,), jnp.float32) < share
    slow_rate = jnp.log(jax.random.uniform(second, (HEADS,), jnp.float32, 0.4, 1.0) / SEQ)
    fast_rate = jax.random.uniform(third, (HEADS,), jnp.float32, jnp.log(1.0 / 60.0), jnp.log(1.0 / 25.0))
    return jnp.where(slowly, slow_rate, fast_rate)


def draw_position_decay_extra(key, part):
    first, second = jax.random.split(jax.random.fold_in(key, 13))
    places = jax.random.randint(first, (3,), 0, SEQ)
    losses = jnp.log(jax.random.uniform(second, (3, HEADS), jnp.float32, 0.5, 0.8))
    positions = jnp.arange(SEQ)
    hits = (positions[:, None] == places[None, :]).astype(jnp.float32)
    return jnp.sum(hits[:, :, None] * losses[None, :, :], axis=1)


def block_levels(rng, dims, cuts, smallest, top_value):
    level = 1.0
    for position, parts in cuts:
        heights = jax.random.uniform(jax.random.fold_in(jax.random.fold_in(rng, 6), position), (parts,), jnp.float32, smallest / len(cuts), top_value / len(cuts))
        level = level * jnp.repeat(jnp.exp(heights), dims[position] // parts).reshape((-1,) + (1,) * (len(dims) - 1 - position))
    return level


def scatter_about(own_key, extent, deviation, bound, pieces=(), held_as=jnp.bfloat16):
    loudness = block_levels(own_key, extent, pieces, -0.22, 0.18) if pieces else 1.0
    array = jax.random.normal(own_key, extent, jnp.float32) * deviation * loudness
    return jnp.minimum(jnp.maximum(array, -bound), bound).astype(held_as)


def setup_inputs(seed: int = 0) -> dict:
    streams_of = jax.random.split(jax.random.key(seed), 21)
    mixer_value_projection = scatter_about(streams_of[0], (SEQ, INNER), 1.0, 6.0, ((0, 32), (1, 4)))
    write_vectors_projected = scatter_about(streams_of[1], (SEQ, GROUPS * STATE), 1.0, 6.0, ((0, 32), (1, 4)))
    read_vectors_projected = scatter_about(streams_of[2], (SEQ, GROUPS * STATE), 1.0, 6.0, ((0, 32), (1, 4)))
    output_gate_projected = scatter_about(streams_of[3], (SEQ, INNER), 1.0, 6.0, ((0, 32), (1, 4)))
    step_size_scores = draw_step_size_scores(jax.random.fold_in(streams_of[20], 71), 0)
    position_decay_extra = draw_position_decay_extra(jax.random.fold_in(streams_of[20], 71), 0)
    step_size_bias = jnp.clip(jax.random.uniform(streams_of[6], (HEADS,), jnp.float32, -1.0, 1.0) * block_levels(streams_of[6], (HEADS,), ((0, 4),), -0.4, 0.0), -1.0, 1.0)
    head_decay_logarithm = draw_head_decay_logarithm(jax.random.fold_in(streams_of[20], 71), 0)
    value_filter_taps = scatter_about(streams_of[8], (CONV_MIX, INNER), CONV_MIX ** -0.5, 3.0, ((1, 4),))
    write_filter_taps = scatter_about(streams_of[9], (CONV_MIX, GROUPS * STATE), CONV_MIX ** -0.5, 3.0, ((1, 4),))
    read_filter_taps = scatter_about(streams_of[10], (CONV_MIX, GROUPS * STATE), CONV_MIX ** -0.5, 3.0, ((1, 4),))
    gated_group_norm_gain = jnp.clip(1.0 + 0.18 * jax.random.normal(streams_of[11], (INNER,), jnp.float32), 0.1, 1.9)
    mixer_output_weight = scatter_about(streams_of[12], (INNER, D), INNER ** -0.5, 0.125, ((0, 4),))
    residual = scatter_about(streams_of[13], (SEQ, D), 1.0, 6.0, ((0, 32),))
    feedforward_norm_gain = jnp.clip(1.0 + 0.18 * jax.random.normal(streams_of[14], (D,), jnp.float32), 0.1, 1.9)
    feedforward_gate_weight = scatter_about(streams_of[15], (D, FF), D ** -0.5, 0.125, ((0, 32), (1, 4)))
    feedforward_value_weight = scatter_about(streams_of[16], (D, FF), D ** -0.5, 0.125, ((0, 32), (1, 4)))
    gate_filter_taps = scatter_about(streams_of[17], (CONV_FFN, FF), CONV_FFN ** -0.5, 3.5, ((1, 4),))
    single_value_filter_taps = scatter_about(streams_of[18], (CONV_FFN, FF), CONV_FFN ** -0.5, 3.5, ((1, 4),))
    feedforward_down_weight = scatter_about(streams_of[19], (FF, D), FF ** -0.5, 0.078125, ((0, 4), (1, 32)))
    return {"mixer_value_projection": mixer_value_projection, "write_vectors_projected": write_vectors_projected, "read_vectors_projected": read_vectors_projected, "output_gate_projected": output_gate_projected, "step_size_scores": step_size_scores, "position_decay_extra": position_decay_extra, "step_size_bias": step_size_bias, "head_decay_logarithm": head_decay_logarithm, "value_filter_taps": value_filter_taps, "write_filter_taps": write_filter_taps, "read_filter_taps": read_filter_taps, "gated_group_norm_gain": gated_group_norm_gain, "mixer_output_weight": mixer_output_weight, "residual": residual, "feedforward_norm_gain": feedforward_norm_gain, "feedforward_gate_weight": feedforward_gate_weight, "feedforward_value_weight": feedforward_value_weight, "gate_filter_taps": gate_filter_taps, "single_value_filter_taps": single_value_filter_taps, "feedforward_down_weight": feedforward_down_weight}


epsilon = 1e-06

def causal_taps(current, kernel):
    tap_count = kernel.shape[0]
    length = current.shape[0]
    padded = jnp.concatenate([jnp.zeros((tap_count - 1, current.shape[1]), current.dtype), current], 0).astype(jnp.float32)
    result = jnp.zeros((length, current.shape[1]), jnp.float32)
    for offset in range(tap_count):
        result = result + kernel[offset].astype(jnp.float32) * padded[offset:offset + length]
    return result

def channel_norm(stream, gain):
    floats = stream.astype(jnp.float32)
    scaled = floats * lax.rsqrt(lax.optimization_barrier(jnp.mean(floats * floats, axis=-1, keepdims=True)) + epsilon)
    return (scaled * gain).astype(jnp.bfloat16)

def reference(mixer_value_projection, write_vectors_projected, read_vectors_projected, output_gate_projected, step_size_scores, position_decay_extra, step_size_bias, head_decay_logarithm, value_filter_taps, write_filter_taps, read_filter_taps, gated_group_norm_gain, mixer_output_weight, residual, feedforward_norm_gain, feedforward_gate_weight, feedforward_value_weight, gate_filter_taps, single_value_filter_taps, feedforward_down_weight):
    per_group = HEADS // GROUPS
    x_conv = jax.nn.silu(causal_taps(mixer_value_projection, value_filter_taps)).astype(jnp.bfloat16)
    write_conv = jax.nn.silu(causal_taps(write_vectors_projected, write_filter_taps)).astype(jnp.bfloat16)
    read_conv = jax.nn.silu(causal_taps(read_vectors_projected, read_filter_taps)).astype(jnp.bfloat16)
    step_size_head = jax.nn.softplus(step_size_scores + step_size_bias)
    logarithm_decay_rate = -step_size_head * jnp.exp(head_decay_logarithm) + position_decay_extra
    scaled = (x_conv.astype(jnp.float32).reshape(SEQ, HEADS, HEAD) * step_size_head[:, :, None]).astype(jnp.bfloat16)
    block_count = SEQ // BLOCK
    value_blocks = scaled.reshape(block_count, BLOCK, GROUPS, per_group, HEAD)
    write_blocks = write_conv.reshape(block_count, BLOCK, GROUPS, STATE)
    read_blocks = read_conv.reshape(block_count, BLOCK, GROUPS, STATE)
    log_blocks = logarithm_decay_rate.reshape(block_count, BLOCK, HEADS)
    causal = jnp.tril(jnp.ones((BLOCK, BLOCK), dtype=jnp.bool_))

    def block_step(carried, inputs):
        value_rows, write_rows, read_rows, log_rows = inputs
        running = jnp.cumsum(log_rows, axis=0)
        by_head = running.T
        spread = by_head[:, :, None] - by_head[:, None, :]
        decays = jnp.exp(jnp.where(causal, spread, -jnp.inf)).reshape(GROUPS, per_group, BLOCK, BLOCK)
        scores = jnp.einsum('lgn,sgn->gls', read_rows.astype(jnp.float32), write_rows.astype(jnp.float32))
        weights = (scores[:, None] * decays).astype(jnp.bfloat16)
        inside = jnp.einsum('grls,sgrp->lgrp', weights.astype(jnp.float32), value_rows.astype(jnp.float32))
        entering = jnp.einsum('lgn,grnp->lgrp', read_rows.astype(jnp.float32), carried, precision=lax.Precision.HIGHEST)
        entering = entering * jnp.exp(running).reshape(BLOCK, GROUPS, per_group)[..., None]
        tails = jnp.exp(by_head[:, -1:] - by_head).T.reshape(BLOCK, GROUPS, per_group)
        tailed = (value_rows.astype(jnp.float32) * tails[..., None]).astype(jnp.bfloat16)
        fresh = jnp.einsum('sgn,sgrp->grnp', write_rows.astype(jnp.float32), tailed.astype(jnp.float32))
        advanced = carried * jnp.exp(running[-1]).reshape(GROUPS, per_group)[..., None, None] + fresh
        return (advanced, inside + entering)
    start_state = jnp.zeros((GROUPS, per_group, STATE, HEAD), jnp.float32)
    outputs = lax.scan(block_step, start_state, (value_blocks, write_blocks, read_blocks, log_blocks))[1]
    mixer = outputs.reshape(SEQ, INNER)
    gated = (mixer * jax.nn.silu(output_gate_projected.astype(jnp.float32))).reshape(SEQ, GROUPS, INNER // GROUPS)
    gated = gated * lax.rsqrt(lax.optimization_barrier(jnp.mean(gated * gated, axis=-1, keepdims=True)) + epsilon)
    normed = (gated.reshape(SEQ, INNER) * gated_group_norm_gain).astype(jnp.bfloat16)
    stream = (residual.astype(jnp.float32) + jnp.dot(normed, mixer_output_weight, preferred_element_type=jnp.float32)).astype(jnp.bfloat16)
    ffn_in = channel_norm(stream, feedforward_norm_gain)
    gate_rows = jnp.dot(ffn_in, feedforward_gate_weight, preferred_element_type=jnp.float32).astype(jnp.bfloat16)
    value_rows = jnp.dot(ffn_in, feedforward_value_weight, preferred_element_type=jnp.float32).astype(jnp.bfloat16)
    hidden = (jax.nn.silu(causal_taps(gate_rows, gate_filter_taps)) * causal_taps(value_rows, single_value_filter_taps)).astype(jnp.bfloat16)
    down = jnp.dot(hidden, feedforward_down_weight, preferred_element_type=jnp.float32)
    return (stream.astype(jnp.float32) + down).astype(jnp.bfloat16)
```

```python
import jax
import jax.numpy as jnp
from jax import lax
from jax.experimental import pallas as pl
from jax.experimental.pallas import tpu as pltpu
from jax.sharding import Mesh
from jax.sharding import PartitionSpec as P


HEAD = 64
STATE = 64
BLOCK = 128
RIM = 16
SP = ("sp_0", "sp_1", "sp_2")
SP_TP = ("sp_0", "sp_1", "sp_2", "tp")
BF = jnp.bfloat16
F32 = jnp.float32
HIGH = lax.Precision.HIGHEST

epsilon = 1e-06


def shifted(value, axis, by, wrap=False):
    length = lax.axis_size(axis)
    if wrap:
        pairs = [(i, (i + by) % length) for i in range(length)]
    else:
        pairs = [(i, i + by) for i in range(length) if 0 <= i + by < length]
    return lax.ppermute(value, axis, pairs)


def swapped(value):
    return lax.ppermute(value, "sp_2", [(0, 1), (1, 0)])


def turned(value, phase, by):
    zs, ys, cs = (lax.axis_size(axis) for axis in SP)
    pairs = []
    for z in range(zs):
        for y in range(ys):
            for c in range(cs):
                to_z, to_y = (z, (y + by) % ys) if c == phase else ((z + by) % zs, y)
                pairs.append(((z * ys + y) * cs + c, (to_z * ys + to_y) * cs + c))
    return lax.ppermute(value, SP, pairs)


def ring_of(step, value):
    half = value.shape[0] // 2
    behind = step(value, 1)
    ahead = step(value, -1)
    far_behind = step(behind[:half], 1)
    far_ahead = step(ahead[half:], -1)
    return behind, ahead, far_behind, far_ahead


def turned_ring(value, phase):
    return ring_of(lambda a, by: turned(a, phase, by), value)


def named_swaps(values):
    result = []
    for value in values:
        result.append(swapped(value))
    return result


def sent_to_all(value, axis):
    length = lax.axis_size(axis)
    return lax.all_to_all(
        jnp.broadcast_to(value[None], (length, *value.shape)), axis, 0, 0, tiled=True
    )


def silu(v):
    return v / (1.0 + jnp.exp(-v))


def rolled_taps(before, current, taps):
    count = taps.shape[0]
    rows = current.shape[0]
    padded = jnp.concatenate([before, current], 0)
    result = taps[count - 1 : count].astype(F32) * current
    for back in range(1, count):
        moved = pltpu.roll(padded, back, 0)[8 : 8 + rows]
        result = result + taps[count - 1 - back : count - back].astype(F32) * moved
    return result


def mixer_kernel(
    x_ref, w_ref, r_ref, hx_ref, hw_ref, hr_ref, dt_ref, ex_ref, bias_ref, rate_ref,
    tx_ref, tw_ref, tr_ref,
    y_ref, read_ref, grow_ref, state_ref,
    carry, total, bx, bw, br,
):
    step_index = pl.program_id(0)
    heads = dt_ref.shape[1]
    inner = x_ref.shape[1]

    @pl.when(step_index == 0)
    def _():
        carry[...] = jnp.zeros_like(carry)
        total[...] = jnp.zeros_like(total)
        bx[...] = hx_ref[RIM - 8 :, :].astype(F32)
        bw[...] = hw_ref[RIM - 8 :, :].astype(F32)
        br[...] = hr_ref[RIM - 8 :, :].astype(F32)

    cx = x_ref[...].astype(F32)
    cw = w_ref[...].astype(F32)
    cr = r_ref[...].astype(F32)
    x = silu(rolled_taps(bx[...], cx, tx_ref[...])).astype(BF)
    write = silu(rolled_taps(bw[...], cw, tw_ref[...])).astype(BF)
    read = silu(rolled_taps(br[...], cr, tr_ref[...])).astype(BF)
    bx[...] = cx[BLOCK - 8 :]
    bw[...] = cw[BLOCK - 8 :]
    br[...] = cr[BLOCK - 8 :]

    spread_of = (
        lax.broadcasted_iota(jnp.int32, (heads, inner), 1) // HEAD
        == lax.broadcasted_iota(jnp.int32, (heads, inner), 0)
    ).astype(F32)

    def spread(a):
        return jnp.dot(a, spread_of, precision=HIGH, preferred_element_type=F32)

    raw = dt_ref[...] + bias_ref[...]
    step = jnp.maximum(raw, 0.0) + jnp.log1p(jnp.exp(-jnp.abs(raw)))
    log_decay = -step * jnp.exp(rate_ref[...]) + ex_ref[...]
    rows = lax.broadcasted_iota(jnp.int32, (BLOCK, BLOCK), 0)
    cols = lax.broadcasted_iota(jnp.int32, (BLOCK, BLOCK), 1)
    causal = rows >= cols
    lower = causal.astype(F32)
    cum = jnp.dot(lower, log_decay, precision=HIGH, preferred_element_type=F32)
    cum_t = lax.dot_general(
        log_decay, lower, (((0,), (1,)), ((), ())), precision=HIGH, preferred_element_type=F32
    )
    scaled = (x.astype(F32) * spread(step)).astype(BF)
    scores = lax.dot_general(
        read, write, (((1,), (1,)), ((), ())), preferred_element_type=F32
    )
    first_half = lax.broadcasted_iota(jnp.int32, (BLOCK, 2 * HEAD), 1) < HEAD
    pieces = []
    for pair in range(heads // 2):
        values = scaled[:, pair * 2 * HEAD : (pair + 1) * 2 * HEAD]
        both = []
        for h in (2 * pair, 2 * pair + 1):
            gap = cum[:, h : h + 1] - cum_t[h : h + 1, :]
            weights = (scores * jnp.exp(jnp.where(causal, gap, -1e30))).astype(BF)
            both.append(jnp.dot(weights, values, preferred_element_type=F32))
        pieces.append(jnp.where(first_half, both[0], both[1]))
    inside = jnp.concatenate(pieces, 1)
    grown = spread(jnp.exp(cum))
    entering = jnp.dot(read.astype(F32), carry[...], precision=HIGH, preferred_element_type=F32)
    y_ref[...] = inside + grown * entering
    read_ref[...] = read
    grow_ref[...] = jnp.exp(cum + total[...][:1])
    tails = jnp.exp(cum[BLOCK - 1 :] - cum)
    tailed = (scaled.astype(F32) * spread(tails)).astype(BF)
    fresh = lax.dot_general(
        write, tailed, (((0,), (0,)), ((), ())), preferred_element_type=F32
    )
    new_state = carry[...] * grown[BLOCK - 1 :] + fresh
    new_total = total[...] + cum[BLOCK - 1 :]
    carry[...] = new_state
    total[...] = new_total

    @pl.when(step_index == pl.num_programs(0) - 1)
    def _():
        state_ref[:STATE, :] = new_state.astype(BF)
        decay = spread(jnp.exp(new_total))
        state_ref[STATE:, :] = jnp.concatenate([decay, decay], 0).astype(BF)


def mixer_local(x, w, r, hx, hw, hr, dt, ex, bias, rate, tx, tw, tr):
    rows, inner = x.shape
    heads = dt.shape[1]
    by_block = lambda width: pl.BlockSpec((BLOCK, width), lambda b: (b, 0))
    whole = lambda a: pl.BlockSpec(a.shape, lambda b: (0, 0))
    return pl.pallas_call(
        mixer_kernel,
        grid=(rows // BLOCK,),
        in_specs=[by_block(inner), by_block(STATE), by_block(STATE)]
        + [whole(a) for a in (hx, hw, hr)]
        + [by_block(heads), by_block(heads)]
        + [whole(a) for a in (bias, rate, tx, tw, tr)],
        out_specs=[
            by_block(inner),
            by_block(STATE),
            by_block(heads),
            pl.BlockSpec((STATE + RIM, inner), lambda b: (0, 0)),
        ],
        out_shape=[
            jax.ShapeDtypeStruct((rows, inner), F32),
            jax.ShapeDtypeStruct((rows, STATE), BF),
            jax.ShapeDtypeStruct((rows, heads), F32),
            jax.ShapeDtypeStruct((STATE + RIM, inner), BF),
        ],
        scratch_shapes=[
            pltpu.VMEM((STATE, inner), F32),
            pltpu.VMEM((8, heads), F32),
            pltpu.VMEM((8, inner), F32),
            pltpu.VMEM((8, STATE), F32),
            pltpu.VMEM((8, STATE), F32),
        ],
        name="mixer_local",
    )(x, w, r, hx, hw, hr, dt, ex, bias, rate, tx, tw, tr)


def finish_kernel(y_ref, read_ref, grow_ref, gate_ref, state_ref, gain_ref, out_ref):
    heads = grow_ref.shape[1]
    inner = y_ref.shape[1]
    spread_of = (
        lax.broadcasted_iota(jnp.int32, (heads, inner), 1) // HEAD
        == lax.broadcasted_iota(jnp.int32, (heads, inner), 0)
    ).astype(F32)
    grown = jnp.dot(grow_ref[...], spread_of, precision=HIGH, preferred_element_type=F32)
    entering = jnp.dot(
        read_ref[...].astype(F32), state_ref[...], precision=HIGH, preferred_element_type=F32
    )
    mixer = y_ref[...] + grown * entering
    gated = mixer * silu(gate_ref[...].astype(F32))
    mean = jnp.mean(gated * gated, axis=-1, keepdims=True)
    out_ref[...] = (gated * lax.rsqrt(mean + epsilon) * gain_ref[...]).astype(BF)


def mixer_finish(y, read, grow, gate, state, gain):
    rows, inner = y.shape
    heads = grow.shape[1]
    size = 256
    by_block = lambda width: pl.BlockSpec((size, width), lambda b: (b, 0))
    whole = lambda a: pl.BlockSpec(a.shape, lambda b: (0, 0))
    return pl.pallas_call(
        finish_kernel,
        grid=(rows // size,),
        in_specs=[by_block(inner), by_block(STATE), by_block(heads), by_block(inner)]
        + [whole(state), whole(gain)],
        out_specs=by_block(inner),
        out_shape=jax.ShapeDtypeStruct((rows, inner), BF),
        name="mixer_finish",
    )(y, read, grow, gate, state, gain)


def split_state(packed):
    packed = packed.astype(F32)
    return packed[..., STATE : STATE + 1, :], packed[..., :STATE, :]


def joined(earlier, later):
    return earlier[0] * later[0], earlier[1] * later[0] + later[1]


def packed_state(pair):
    decay = jnp.broadcast_to(pair[0], (RIM, pair[0].shape[1]))
    return jnp.concatenate([pair[1], decay], 0).astype(BF)


def state_before(packed):
    own = split_state(packed)
    other = split_state(swapped(packed))
    late = lax.axis_index("sp_2") == 1
    first = jax.tree.map(lambda a, b: jnp.where(late, a, b), other, own)
    second = jax.tree.map(lambda a, b: jnp.where(late, a, b), own, other)
    running = joined(first, second)
    before = (
        jnp.where(late, other[0], 1.0),
        jnp.where(late, other[1], 0.0),
    )
    for axis in ("sp_1", "sp_0"):
        here = lax.axis_index(axis)
        all_of = sent_to_all(packed_state(running), axis)
        decay, state = split_state(all_of)
        whole = (jnp.ones_like(decay[0]), jnp.zeros_like(state[0]))
        inside = whole
        for k in range(lax.axis_size(axis)):
            whole = joined(whole, (decay[k], state[k]))
            passed = k < here
            inside = jax.tree.map(lambda new, old: jnp.where(passed, new, old), whole, inside)
        before = joined(inside, before)
        running = whole
    return before[1]


def gathered_ring(value, axis):
    return ring_of(lambda a, by: shifted(a, axis, by, True), value)


def summed_ring(here, on, back, far_on, far_back, axis):
    half = far_on.shape[0]
    more_on = shifted(far_on, axis, 1, True)
    more_back = shifted(far_back, axis, -1, True)
    on = jnp.concatenate(
        [(on[:half].astype(F32) + more_on.astype(F32)).astype(BF), on[half:]], 0
    )
    back = jnp.concatenate(
        [back[:half], (back[half:].astype(F32) + more_back.astype(F32)).astype(BF)], 0
    )
    from_behind = shifted(on, axis, 1, True)
    from_ahead = shifted(back, axis, -1, True)
    return here.astype(F32) + from_behind.astype(F32) + from_ahead.astype(F32)


def rolled(rows, taps):
    count = taps.shape[0]
    result = taps[count - 1 : count] * rows
    for back in range(1, count):
        result = result + taps[count - 1 - back : count - back] * pltpu.roll(rows, back, 0)
    return result


HOPS = (0, -1, 1, 2)


def ffn_kernel(
    place_ref, p0, p1, p2, p3a, p3b, halo, res_ref, hres_ref,
    o0, ob, oa, ofb, ofa, tb, ta, tfb, tfa,
    w0, wb, wa, wfb, wfa, s0, sb, sa, sfb, sfa,
    gain_ref, tg_ref, tv_ref,
    q0, q1, q3, q2a, q2b, own_ref,
    x, wo, wall, stream, xin, hid, part, sem_x, sem_o, sem_w, sem_q,
):
    z_index = place_ref[0]
    y_index = place_ref[1]
    core = place_ref[2]
    tp_index = place_ref[3]
    rows = res_ref.shape[0]
    width = res_ref.shape[1]
    inner = p0.shape[1]
    units = hid.shape[1]
    half = inner // 2
    copies_x, copies_o, copies_w = [], [], []

    def go(into, src, dst, sems):
        copy = pltpu.make_async_copy(src, dst, sems.at[len(into)])
        copy.start()
        into.append(copy)

    for k, by in enumerate(HOPS):
        at = lax.rem(tp_index + (by + 4), 4)
        columns = pl.ds(k * inner, inner)
        if k < 3:
            go(copies_x, (p0, p1, p2)[k], x.at[pl.ds(RIM, rows), columns], sem_x)
        else:
            go(copies_x, p3a, x.at[pl.ds(RIM, rows // 2), columns], sem_x)
            go(copies_x, p3b, x.at[pl.ds(RIM + rows // 2, rows // 2), columns], sem_x)
        go(copies_x, halo.at[at], x.at[pl.ds(0, RIM), columns], sem_x)
    go(copies_o, o0, wo.at[pl.ds(0, inner)], sem_o)
    for side, (b, a, fb, fa) in ((core, (ob, oa, ofb, ofa)), (1 - core, (tb, ta, tfb, tfa))):
        first = pl.multiple_of(side * half, half)
        go(copies_o, b, wo.at[pl.ds(inner + first, half)], sem_o)
        go(copies_o, a, wo.at[pl.ds(2 * inner + first, half)], sem_o)
        go(copies_o, fb, wo.at[pl.ds(3 * inner + first, half // 2)], sem_o)
        go(copies_o, fa, wo.at[pl.ds(3 * inner + first + half // 2, half // 2)], sem_o)
    for side, (o, b, a, fb, fa) in (
        (core, (w0, wb, wa, wfb, wfa)),
        (1 - core, (s0, sb, sa, sfb, sfa)),
    ):
        first_axis = jnp.where(side == 0, y_index, z_index)
        second_axis = jnp.where(side == 0, z_index, y_index)
        for m, by_second in enumerate(HOPS):
            second = lax.rem(second_axis + (by_second + 4), 4)
            for k, by_first in enumerate(HOPS):
                first = lax.rem(first_axis + (by_first + 4), 4)
                chip = jnp.where(side == 0, second * 4 + first, first * 4 + second)
                if m < 3:
                    src = (o, b, a)[m].at[k]
                else:
                    src = (fb, fa)[k // 2].at[k % 2]
                go(copies_w, src, wall.at[chip, :, side], sem_w)

    for copy in copies_x:
        copy.wait()
    for copy in copies_o:
        copy.wait()
    squares = jnp.zeros((rows + RIM, 1), F32)
    blocks = width // 512
    for n in range(blocks):
        columns = slice(n * 512, (n + 1) * 512)
        before = jnp.concatenate([hres_ref[:, columns], res_ref[:, columns]], 0).astype(F32)
        total = before + jnp.dot(x[...], wo[:, columns], preferred_element_type=F32)
        kept = total.astype(BF)
        stream[:, columns] = kept
        wide = kept.astype(F32)
        squares = squares + jnp.sum(wide * wide, axis=-1, keepdims=True)
    scale = lax.rsqrt(squares / width + epsilon)
    for n in range(blocks):
        columns = slice(n * 512, (n + 1) * 512)
        xin[:, columns] = (
            stream[:, columns].astype(F32) * scale * gain_ref[:, columns]
        ).astype(BF)
    share = rows // 4
    own_ref[...] = stream[pl.ds(pl.multiple_of(RIM + tp_index * share, 16), share), :]

    for copy in copies_w:
        copy.wait()
    for at in range(0, units, 384):
        size = min(384, units - at)
        columns = slice(at, at + size)
        gate_weight = wall[..., at : at + size].reshape(width, size)
        value_weight = wall[..., units + at : units + at + size].reshape(width, size)
        gate = jnp.dot(xin[...], gate_weight, preferred_element_type=F32).astype(BF)
        value = jnp.dot(xin[...], value_weight, preferred_element_type=F32).astype(BF)
        gate = rolled(gate.astype(F32), tg_ref[:, columns].astype(F32))
        value = rolled(value.astype(F32), tv_ref[:, columns].astype(F32))
        hid[:, columns] = (silu(gate) * value)[RIM:].astype(BF)

    chips = wall.shape[0] // blocks
    for n in range(blocks):
        down_weight = wall[n * chips : (n + 1) * chips, :, :, :, 2 * units :].reshape(512, units)
        part[:, n * 512 : (n + 1) * 512] = lax.dot_general(
            hid[...], down_weight, (((1,), (1,)), ((), ())), preferred_element_type=F32
        ).astype(BF)
    copies_q = []
    for k, dst in ((2, None), (1, q1), (3, q3), (0, q0)):
        first = pl.multiple_of(lax.rem(tp_index + k, 4) * share, 16)
        if dst is None:
            go(copies_q, part.at[pl.ds(first, share // 2)], q2a, sem_q)
            go(copies_q, part.at[pl.ds(first + share // 2, share // 2)], q2b, sem_q)
        else:
            go(copies_q, part.at[pl.ds(first, share)], dst, sem_q)
    for copy in copies_q:
        copy.wait()


def ffn(place, pieces, halo, residual, hres, out_weights, weights, gain, tg, tv):
    rows, width = residual.shape
    units = tg.shape[1]
    share = rows // 4
    hbm = pl.BlockSpec(memory_space=pl.ANY)
    vmem = pl.BlockSpec(memory_space=pltpu.VMEM)
    smem = pl.BlockSpec(memory_space=pltpu.SMEM)
    shape = jax.ShapeDtypeStruct
    return pl.pallas_call(
        ffn_kernel,
        in_specs=[smem] + [hbm] * 6 + [vmem] * 2 + [hbm] * 19 + [vmem] * 3,
        out_specs=[hbm] * 5 + [vmem],
        out_shape=[shape((share, width), BF)] * 3
        + [shape((share // 2, width), BF)] * 2
        + [shape((share, width), BF)],
        scratch_shapes=[
            pltpu.VMEM((rows + RIM, width), BF),
            pltpu.VMEM((width, width), BF),
            pltpu.VMEM((16, 2, 2, width // 64, 3 * units), BF),
            pltpu.VMEM((rows + RIM, width), BF),
            pltpu.VMEM((rows + RIM, width), BF),
            pltpu.VMEM((rows, units), BF),
            pltpu.VMEM((rows, width), BF),
            pltpu.SemaphoreType.DMA((9,)),
            pltpu.SemaphoreType.DMA((9,)),
            pltpu.SemaphoreType.DMA((32,)),
            pltpu.SemaphoreType.DMA((5,)),
        ],
        compiler_params=pltpu.CompilerParams(vmem_limit_bytes=60 * 1024 * 1024),
        name="ffn",
    )(place, *pieces, halo, residual, hres, *out_weights, *weights, gain, tg, tv)


def on_device(
    mixer_value_projection,
    write_vectors_projected,
    read_vectors_projected,
    output_gate_projected,
    step_size_scores,
    position_decay_extra,
    step_size_bias,
    head_decay_logarithm,
    value_filter_taps,
    write_filter_taps,
    read_filter_taps,
    gated_group_norm_gain,
    mixer_output_weight,
    residual,
    feedforward_norm_gain,
    feedforward_gate_weight,
    feedforward_value_weight,
    gate_filter_taps,
    single_value_filter_taps,
    feedforward_down_weight,
):
    row_count, inner = mixer_value_projection.shape
    core = lax.axis_index("sp_2")
    tp_index = lax.axis_index("tp")

    rows = jnp.concatenate(
        [feedforward_gate_weight, feedforward_value_weight, feedforward_down_weight.T], 1
    )
    part = rows.shape[0] // 2
    keep = jnp.where(core == 0, rows[:part], rows[part:])
    got = swapped(jnp.where(core == 0, rows[part:], rows[:part]))
    piece = jnp.concatenate([jnp.where(core == 0, keep, got), jnp.where(core == 0, got, keep)], 0)
    line = jnp.concatenate([piece, *turned_ring(piece, 0)], 0)
    plane = [line, *turned_ring(line, 1)]
    plane = [a.reshape(-1, 2, part, a.shape[1]) for a in plane]
    weights = [*plane, *named_swaps(plane)]

    own_half = lax.dynamic_slice_in_dim(mixer_output_weight, core * (inner // 2), inner // 2, 0)
    out_ring = gathered_ring(own_half, "tp")
    out_weights = [mixer_output_weight, *out_ring, *named_swaps(out_ring)]

    rim = jnp.concatenate(
        [
            a[row_count - RIM :]
            for a in (
                mixer_value_projection,
                write_vectors_projected,
                read_vectors_projected,
                residual,
            )
        ],
        1,
    )
    rim = shifted(rim, SP, 1)
    y, read, grow, packed = mixer_local(
        mixer_value_projection,
        write_vectors_projected,
        read_vectors_projected,
        rim[:, :inner],
        rim[:, inner : inner + STATE],
        rim[:, inner + STATE : inner + 2 * STATE],
        step_size_scores,
        position_decay_extra,
        step_size_bias[None],
        head_decay_logarithm[None],
        value_filter_taps,
        write_filter_taps,
        read_filter_taps,
    )
    state = state_before(packed)
    normed = mixer_finish(y, read, grow, output_gate_projected, state, gated_group_norm_gain[None])

    pieces = [normed, *gathered_ring(normed, "tp")]
    halo = shifted(normed[row_count - RIM :], SP, 1)
    halo = sent_to_all(halo, "tp")
    places = [lax.axis_index("sp_0"), lax.axis_index("sp_1"), core, tp_index]
    q0, q1, q3, q2a, q2b, own = ffn(
        jnp.stack(places).astype(jnp.int32),
        pieces,
        halo,
        residual,
        rim[:, inner + 2 * STATE :],
        out_weights,
        weights,
        feedforward_norm_gain[None],
        gate_filter_taps,
        single_value_filter_taps,
    )
    down = summed_ring(q0, q1, q3, q2a, q2b, "tp")
    return (own.astype(F32) + down).astype(BF)


def solution(mesh):
    torus = Mesh(mesh.devices.reshape(4, 4, 2, mesh.shape["tp"]), ("sp_0", "sp_1", "sp_2", "tp"))
    in_specs = (
        P(SP, "tp"),
        P(SP, "tp"),
        P(SP, "tp"),
        P(SP, "tp"),
        P(SP, "tp"),
        P(SP, "tp"),
        P("tp"),
        P("tp"),
        P(None, "tp"),
        P(None, "tp"),
        P(None, "tp"),
        P("tp"),
        P("tp", None),
        P(SP, None),
        P(),
        P(SP, "tp"),
        P(SP, "tp"),
        P(None, "tp"),
        P(None, "tp"),
        P("tp", SP),
    )
    out_specs = P(SP_TP, None)

    return jax.shard_map(
        on_device, mesh=torus, in_specs=in_specs, out_specs=out_specs, check_vma=False
    )
```

```python
import jax
import jax.numpy as jnp
from jax import lax
from jax.experimental import pallas as pl
from jax.experimental.pallas import tpu as pltpu
from jax.sharding import Mesh
from jax.sharding import PartitionSpec as P


HEAD = 64
STATE = 64
BLOCK = 128
RIM = 16
SP = ("sp_0", "sp_1", "sp_2")
SP_TP = ("sp_0", "sp_1", "sp_2", "tp")
BF = jnp.bfloat16
F32 = jnp.float32

epsilon = 1e-06


def shifted(value, axis, by, wrap=False):
    length = lax.axis_size(axis)
    if wrap:
        pairs = [(i, (i + by) % length) for i in range(length)]
    else:
        pairs = [(i, i + by) for i in range(length) if 0 <= i + by < length]
    return lax.ppermute(value, axis, pairs)


def swapped(value):
    return lax.ppermute(value, "sp_2", [(0, 1), (1, 0)])


def turned(value, phase, by):
    zs, ys, cs = (lax.axis_size(axis) for axis in SP)
    pairs = []
    for z in range(zs):
        for y in range(ys):
            for c in range(cs):
                to_z, to_y = (z, (y + by) % ys) if c == phase else ((z + by) % zs, y)
                pairs.append(((z * ys + y) * cs + c, (to_z * ys + to_y) * cs + c))
    return lax.ppermute(value, SP, pairs)


def short_ring(step, value):
    behind = step(value, 1)
    ahead = step(value, -1)
    far = step(behind, 1)
    return behind, ahead, far


def named_swaps(values):
    result = []
    for value in values:
        result.append(swapped(value))
    return result


def sent_to_all(value, axis):
    length = lax.axis_size(axis)
    return lax.all_to_all(
        jnp.broadcast_to(value[None], (length, *value.shape)), axis, 0, 0, tiled=True
    )


def silu(v):
    return v / (1.0 + jnp.exp(-v))


def rolled_taps(before, current, taps):
    count = taps.shape[0]
    rows = current.shape[0]
    padded = jnp.concatenate([before, current], 0)
    result = taps[count - 1 : count].astype(F32) * current
    for back in range(1, count):
        moved = pltpu.roll(padded, back, 0)[8 : 8 + rows]
        result = result + taps[count - 1 - back : count - back].astype(F32) * moved
    return result


def halves(a, axis):
    high = a.astype(BF)
    return jnp.concatenate([high, (a - high.astype(F32)).astype(BF)], axis)


def thirds(a, axis):
    high = a.astype(BF)
    rest = a - high.astype(F32)
    middle = rest.astype(BF)
    return jnp.concatenate([high, middle, (rest - middle.astype(F32)).astype(BF)], axis)


def head_lanes(heads, inner):
    one = (
        lax.broadcasted_iota(jnp.int32, (heads, inner), 1) // HEAD
        == lax.broadcasted_iota(jnp.int32, (heads, inner), 0)
    ).astype(F32)
    return jnp.concatenate([one, one], 0).astype(BF)


def spread(by_head, lanes):
    return lax.dot_general(
        halves(by_head, 0), lanes, (((0,), (0,)), ((), ())), preferred_element_type=F32
    )


def mixer_kernel(
    x_ref, w_ref, r_ref, rim_ref, dt_ref, ex_ref, bias_ref, rate_ref,
    tx_ref, tw_ref, tr_ref,
    scaled_ref, write_ref, read_ref, before_ref, cum_ref, grow_ref, state_ref,
    carry, total, bx, bw, br,
):
    step_index = pl.program_id(0)
    heads = dt_ref.shape[0]
    size, inner = x_ref.shape

    @pl.when(step_index == 0)
    def _():
        carry[...] = jnp.zeros_like(carry)
        total[...] = jnp.zeros_like(total)
        rim = rim_ref[RIM - 8 :, : inner + 2 * STATE].astype(F32)
        bx[...] = rim[:, :inner]
        bw[...] = rim[:, inner : inner + STATE]
        br[...] = rim[:, inner + STATE :]

    cx = x_ref[...].astype(F32)
    cw = w_ref[...].astype(F32).T
    cr = r_ref[...].astype(F32).T
    x = silu(rolled_taps(bx[...], cx, tx_ref[...])).astype(BF)
    write = silu(rolled_taps(bw[...], cw, tw_ref[...])).astype(BF)
    read = silu(rolled_taps(br[...], cr, tr_ref[...])).astype(BF)
    bx[...] = cx[size - 8 :]
    bw[...] = cw[size - 8 :]
    br[...] = cr[size - 8 :]
    write_ref[...] = write
    read_ref[...] = read

    lanes = head_lanes(heads, inner)
    column = lambda a: jnp.broadcast_to(a, (heads, heads)).T[:, :1]
    raw = dt_ref[...] + column(bias_ref[...])
    step = jnp.maximum(raw, 0.0) + jnp.log1p(jnp.exp(-jnp.abs(raw)))
    log_decay = -step * jnp.exp(column(rate_ref[...])) + ex_ref[...]
    upper = (
        lax.broadcasted_iota(jnp.int32, (BLOCK, BLOCK), 0)
        <= lax.broadcasted_iota(jnp.int32, (BLOCK, BLOCK), 1)
    ).astype(F32).astype(BF)
    state = carry[...]
    sum_before = total[...]
    scaled = (x.astype(F32) * spread(step, lanes)).astype(BF)
    scaled_ref[...] = scaled
    for k in range(size // BLOCK):
        here = slice(k * BLOCK, (k + 1) * BLOCK)
        parts = jnp.dot(thirds(log_decay[:, here], 0), upper, preferred_element_type=F32)
        cum = parts[:heads] + parts[heads : 2 * heads] + parts[2 * heads :]
        end = cum[:, BLOCK - 1 :]
        cum_ref[:, here] = cum
        grow_ref[:, here] = jnp.exp(cum + sum_before[:, :1])
        before_ref[k * STATE : (k + 1) * STATE, :] = state
        tails = spread(jnp.exp(end - cum), lanes)
        tailed = (scaled[here].astype(F32) * tails).astype(BF)
        fresh = lax.dot_general(
            write[here], tailed, (((0,), (0,)), ((), ())), preferred_element_type=F32
        )
        decay = spread(jnp.broadcast_to(jnp.exp(end), (heads, BLOCK)), lanes)
        state = state * decay[:1] + fresh
        sum_before = sum_before + end
    carry[...] = state
    total[...] = sum_before

    @pl.when(step_index == pl.num_programs(0) - 1)
    def _():
        state_ref[:STATE, :] = state.astype(BF)
        decay = spread(jnp.exp(sum_before), lanes)
        state_ref[STATE:, :] = decay[:RIM].astype(BF)


def mixer_local(x, w, r, rim, dt, ex, bias, rate, tx, tw, tr):
    rows, inner = x.shape
    heads = dt.shape[0]
    size = 2 * BLOCK
    by_block = lambda width: pl.BlockSpec((size, width), lambda b: (b, 0))
    by_lanes = pl.BlockSpec((heads, size), lambda b: (0, b))
    by_channel = pl.BlockSpec((STATE, size), lambda b: (0, b))
    whole = lambda a: pl.BlockSpec(a.shape, lambda b: (0, 0))
    shape = jax.ShapeDtypeStruct
    blocks = rows // BLOCK
    return pl.pallas_call(
        mixer_kernel,
        grid=(rows // size,),
        in_specs=[by_block(inner), by_channel, by_channel, whole(rim), by_lanes, by_lanes]
        + [whole(a) for a in (bias, rate, tx, tw, tr)],
        out_specs=[
            by_block(inner),
            by_block(STATE),
            by_block(STATE),
            pl.BlockSpec((size // BLOCK * STATE, inner), lambda b: (b, 0)),
            by_lanes,
            by_lanes,
            pl.BlockSpec((STATE + RIM, inner), lambda b: (0, 0)),
        ],
        out_shape=[
            shape((rows, inner), BF),
            shape((rows, STATE), BF),
            shape((rows, STATE), BF),
            shape((blocks * STATE, inner), F32),
            shape((heads, rows), F32),
            shape((heads, rows), F32),
            shape((STATE + RIM, inner), BF),
        ],
        scratch_shapes=[
            pltpu.VMEM((STATE, inner), F32),
            pltpu.VMEM((heads, BLOCK), F32),
            pltpu.VMEM((8, inner), F32),
            pltpu.VMEM((8, STATE), F32),
            pltpu.VMEM((8, STATE), F32),
        ],
        name="mixer_local",
    )(x, w, r, rim, dt, ex, bias, rate, tx, tw, tr)


def entered(read, state):
    return jnp.dot(
        jnp.concatenate([read, read], 1), halves(state, 0), preferred_element_type=F32
    )


def inside_kernel(scaled_ref, write_ref, read_ref, before_ref, cum_ref, y_ref):
    heads = cum_ref.shape[0]
    size, inner = scaled_ref.shape
    lanes = head_lanes(heads, inner)
    rows = lax.broadcasted_iota(jnp.int32, (BLOCK, BLOCK), 0)
    cols = lax.broadcasted_iota(jnp.int32, (BLOCK, BLOCK), 1)
    causal = rows >= cols
    first_half = lax.broadcasted_iota(jnp.int32, (BLOCK, 2 * HEAD), 1) < HEAD
    for k in range(size // BLOCK):
        here = slice(k * BLOCK, (k + 1) * BLOCK)
        read = read_ref[here, :]
        scaled = scaled_ref[here, :]
        cum_t = cum_ref[:, here]
        cum = cum_t.T
        scores = lax.dot_general(
            read, write_ref[here, :], (((1,), (1,)), ((), ())), preferred_element_type=F32
        )
        pieces = []
        for pair in range(heads // 2):
            values = scaled[:, pair * 2 * HEAD : (pair + 1) * 2 * HEAD]
            both = []
            for h in (2 * pair, 2 * pair + 1):
                gap = cum[:, h : h + 1] - cum_t[h : h + 1, :]
                both.append((scores * jnp.exp(jnp.where(causal, gap, -1e30))).astype(BF))
            product = jnp.dot(jnp.concatenate(both, 0), values, preferred_element_type=F32)
            pieces.append(jnp.where(first_half, product[:BLOCK], product[BLOCK:]))
        before = before_ref[k * STATE : (k + 1) * STATE, :]
        grown = spread(jnp.exp(cum_t), lanes)
        y_ref[here, :] = jnp.concatenate(pieces, 1) + grown * entered(read, before)


def mixer_inside(scaled, write, read, before, cum):
    rows, inner = scaled.shape
    heads = cum.shape[0]
    size = 2 * BLOCK
    by_block = lambda width: pl.BlockSpec((size, width), lambda b: (b, 0))
    return pl.pallas_call(
        inside_kernel,
        grid=(rows // size,),
        in_specs=[
            by_block(inner),
            by_block(STATE),
            by_block(STATE),
            pl.BlockSpec((size // BLOCK * STATE, inner), lambda b: (b, 0)),
            pl.BlockSpec((heads, size), lambda b: (0, b)),
        ],
        out_specs=by_block(inner),
        out_shape=jax.ShapeDtypeStruct((rows, inner), F32),
        name="mixer_inside",
    )(scaled, write, read, before, cum)


def finish_kernel(y_ref, read_ref, grow_ref, gate_ref, state_ref, gain_ref, top_ref, low_ref):
    grown = spread(grow_ref[...], head_lanes(grow_ref.shape[0], y_ref.shape[1]))
    mixer = y_ref[...] + grown * entered(read_ref[...], state_ref[...])
    gated = mixer * silu(gate_ref[...].astype(F32))
    mean = jnp.mean(gated * gated, axis=-1, keepdims=True)
    normed = (gated * lax.rsqrt(mean + epsilon) * gain_ref[...]).astype(BF)

    @pl.when(pl.program_id(0) == 0)
    def _():
        top_ref[...] = normed

    @pl.when(pl.program_id(0) == 1)
    def _():
        low_ref[...] = normed


def mixer_finish(y, read, grow, gate, state, gain):
    rows, inner = y.shape
    heads = grow.shape[0]
    size = rows // 2
    by_block = lambda width: pl.BlockSpec((size, width), lambda b: (b, 0))
    whole = lambda a: pl.BlockSpec(a.shape, lambda b: (0, 0))
    return pl.pallas_call(
        finish_kernel,
        grid=(rows // size,),
        in_specs=[by_block(inner), by_block(STATE), pl.BlockSpec((heads, size), lambda b: (0, b))]
        + [by_block(inner), whole(state), whole(gain)],
        out_specs=[pl.BlockSpec((size, inner), lambda b: (0, 0))] * 2,
        out_shape=[jax.ShapeDtypeStruct((size, inner), BF)] * 2,
        name="mixer_finish",
    )(y, read, grow, gate, state, gain)


def split_state(packed):
    packed = packed.astype(F32)
    return packed[..., STATE : STATE + 1, :], packed[..., :STATE, :]


def joined(earlier, later):
    return earlier[0] * later[0], earlier[1] * later[0] + later[1]


def packed_state(pair):
    decay = jnp.broadcast_to(pair[0], (RIM, pair[0].shape[1]))
    return jnp.concatenate([pair[1], decay], 0).astype(BF)


def state_before(packed):
    own = split_state(packed)
    other = split_state(swapped(packed))
    late = lax.axis_index("sp_2") == 1
    first = jax.tree.map(lambda a, b: jnp.where(late, a, b), other, own)
    second = jax.tree.map(lambda a, b: jnp.where(late, a, b), own, other)
    running = joined(first, second)
    before = (
        jnp.where(late, other[0], 1.0),
        jnp.where(late, other[1], 0.0),
    )
    for axis in ("sp_1", "sp_0"):
        here = lax.axis_index(axis)
        all_of = sent_to_all(packed_state(running), axis)
        decay, state = split_state(all_of)
        whole = (jnp.ones_like(decay[0]), jnp.zeros_like(state[0]))
        inside = whole
        for k in range(lax.axis_size(axis)):
            whole = joined(whole, (decay[k], state[k]))
            passed = k < here
            inside = jax.tree.map(lambda new, old: jnp.where(passed, new, old), whole, inside)
        before = joined(inside, before)
        running = whole
    return before[1]


def halved_ring(step, top, low):
    result = {}
    for key, value, by in (
        ("bt", top, 1), ("al", low, -1), ("bl", low, 1), ("at", top, -1),
    ):
        result[key] = step(value, by)
    far_top = step(result["bt"], 1)
    far_low = step(result["al"], -1)
    return [
        top, low, result["bt"], result["bl"], result["at"], result["al"], far_top, far_low,
    ]


def rolled(rows, taps):
    count = taps.shape[0]
    result = taps[count - 1 : count] * rows
    for back in range(1, count):
        result = result + taps[count - 1 - back : count - back] * pltpu.roll(rows, back, 0)
    return result


HOPS = (0, -1, 1, 2)


BAND = 512


def go(into, src, dst, sems):
    copy = pltpu.make_async_copy(src, dst, sems.at[len(into)])
    copy.start()
    into.append(copy)


def near_kernel(
    place_ref, p0, l0, p1, l1, p2, l2, halo, res, rim, o0, ob, oa, of, tb, ta, tf,
    total_out,
    x, wo, stream, total, sem_x, sem_o, sem_t,
):
    core = place_ref[2]
    tp_index = place_ref[3]
    rows, width = res.shape
    inner = p0.shape[1]
    half = inner // 2
    near = 3 * inner
    copies_x, copies_o, copies_t = [], [], []
    for k, by in enumerate(HOPS):
        at = lax.rem(tp_index + (by + 4), 4)
        columns = pl.ds(k * inner, inner)
        if k < 3:
            top, low = ((p0, l0), (p1, l1), (p2, l2))[k]
            go(copies_x, top, x.at[pl.ds(RIM, rows // 2), columns], sem_x)
            go(copies_x, low, x.at[pl.ds(RIM + rows // 2, rows // 2), columns], sem_x)
        go(copies_x, halo.at[at], x.at[pl.ds(0, RIM), columns], sem_x)
    bands = width // BAND

    def out_weight(n):
        columns = pl.ds(n * BAND, BAND)
        go(copies_o, o0.at[:, columns], wo.at[pl.ds(0, inner), columns], sem_o)
        for side, pieces in ((core, (ob, oa, of)), (1 - core, (tb, ta, tf))):
            first = pl.multiple_of(side * half, half)
            for k, src in enumerate(pieces):
                into = pl.ds((k + 1) * inner + first, half)
                go(copies_o, src.at[:, columns], wo.at[into, columns], sem_o)

    out_weight(0)
    go(copies_x, rim.at[:, pl.ds(rim.shape[1] - width, width)], stream.at[pl.ds(0, RIM)], sem_x)
    go(copies_x, res, stream.at[pl.ds(RIM, rows)], sem_x)
    for copy in copies_x:
        copy.wait()
    for n in range(1, bands):
        out_weight(n)
    for n in range(bands):
        for copy in copies_o[7 * n : 7 * (n + 1)]:
            copy.wait()
        columns = slice(n * BAND, (n + 1) * BAND)
        total[:, columns] = stream[:, columns].astype(F32) + jnp.dot(
            x[:, :near], wo[:near, columns], preferred_element_type=F32
        )
        total[:RIM, columns] += jnp.dot(
            x[:RIM, near:], wo[near:, columns], preferred_element_type=F32
        )
        go(copies_t, total.at[:, pl.ds(n * BAND, BAND)], total_out.at[:, pl.ds(n * BAND, BAND)], sem_t)
    for copy in copies_t:
        copy.wait()


def out_near(place, pieces, halo, residual, rim, out_weights):
    rows, width = residual.shape
    hbm = pl.BlockSpec(memory_space=pl.ANY)
    return pl.pallas_call(
        near_kernel,
        in_specs=[pl.BlockSpec(memory_space=pltpu.SMEM)] + [hbm] * 16,
        out_specs=hbm,
        out_shape=jax.ShapeDtypeStruct((rows + RIM, width), F32),
        scratch_shapes=[
            pltpu.VMEM((rows + RIM, width), BF),
            pltpu.VMEM((width, width), BF),
            pltpu.VMEM((rows + RIM, width), BF),
            pltpu.VMEM((rows + RIM, width), F32),
            pltpu.SemaphoreType.DMA((12,)),
            pltpu.SemaphoreType.DMA((28,)),
            pltpu.SemaphoreType.DMA((4,)),
        ],
        compiler_params=pltpu.CompilerParams(vmem_limit_bytes=60 * 1024 * 1024),
        name="out_near",
    )(place, *pieces, halo, residual, rim, *out_weights)


UNIT = 256


def unit_blocks(units):
    return [(at, min(UNIT, units - at)) for at in range(0, units, UNIT)]


def weight_copies(place_ref, plane, wall, sems, units):
    z_index = place_ref[0]
    y_index = place_ref[1]
    core = place_ref[2]
    every = []
    stretches = ((0, 2 * UNIT), (2 * UNIT, 2 * units), (2 * units, 3 * units))

    def start(stretch):
        lanes = pl.ds(stretches[stretch][0], stretches[stretch][1] - stretches[stretch][0])
        done = len(every)
        for side, sources in ((core, plane[:8]), (1 - core, plane[8:])):
            first_axis = jnp.where(side == 0, y_index, z_index)
            second_axis = jnp.where(side == 0, z_index, y_index)
            for m, by_second in enumerate(HOPS):
                second = lax.rem(second_axis + (by_second + 4), 4)
                for k, by_first in enumerate((0, -1, 1, 2)):
                    first = lax.rem(first_axis + (by_first + 4), 4)
                    chip = jnp.where(side == 0, second * 4 + first, first * 4 + second)
                    src = sources[2 * m + k // 2].at[k % 2, :, :, lanes]
                    go(every, src, wall.at[chip, :, side, :, lanes], sems)
        return every[done:]

    return start


def ffn_blocks(xin, wall, hid, part, tg_ref, tv_ref, arrived, start, stored):
    width = xin.shape[1]
    units = hid.shape[1]
    for j, (at, size) in enumerate(unit_blocks(units)):
        if j < 2:
            for copy in arrived[j]:
                copy.wait()
        if j == 0:
            arrived.append(start(2))
        weight = wall[..., 2 * at : 2 * (at + size)].reshape(width, 2 * size)
        rows = jnp.dot(xin[...], weight, preferred_element_type=F32).astype(BF).astype(F32)
        taps = jnp.concatenate([tg_ref[:, at : at + size], tv_ref[:, at : at + size]], 1)
        rows = rolled(rows, taps.astype(F32))
        act = (silu(rows[:, :size]) * rows[:, size:]).astype(BF)
        hid[:, at : at + size] = act[RIM:]
    for copy in arrived[2]:
        copy.wait()
    bands = width // BAND
    chips = wall.shape[0] // bands
    for n in range(bands):
        weight = wall[n * chips : (n + 1) * chips, :, :, :, 2 * units :].reshape(BAND, units)
        part[:, n * BAND : (n + 1) * BAND] = lax.dot_general(
            hid[...], weight, (((1,), (1,)), ((), ())), preferred_element_type=F32
        ).astype(BF)
        stored(n)


def ffn_kernel(
    place_ref, p3a, p3b, total_in, of, tf,
    w0, w1, w2, w3, w4, w5, w6, w7, s0, s1, s2, s3, s4, s5, s6, s7,
    gain_ref, tg_ref, tv_ref,
    q0, q1, q3, qa, qb, own_ref,
    p3, wo, total, wall, stream, xin, hid, part, sem_x, sem_t, sem_w, sem_q,
):
    core = place_ref[2]
    tp_index = place_ref[3]
    rows, inner = p3.shape
    width = wo.shape[1]
    units = hid.shape[1]
    half = inner // 2
    share = rows // 4
    bands = width // BAND
    copies_x, copies_t, copies_q = [], [], []
    go(copies_x, p3a, p3.at[pl.ds(0, rows // 2)], sem_x)
    go(copies_x, p3b, p3.at[pl.ds(rows // 2, rows // 2)], sem_x)
    go(copies_x, of, wo.at[pl.ds(pl.multiple_of(core * half, half), half)], sem_x)
    go(copies_x, tf, wo.at[pl.ds(pl.multiple_of((1 - core) * half, half), half)], sem_x)
    for n in range(bands):
        columns = pl.ds(n * BAND, BAND)
        go(copies_t, total_in.at[:, columns], total.at[:, columns], sem_t)
    for copy in copies_x:
        copy.wait()
    squares = jnp.zeros((rows + RIM, 1), F32)
    for n in range(bands):
        copies_t[n].wait()
        if n == 1:
            plane = (w0, w1, w2, w3, w4, w5, w6, w7, s0, s1, s2, s3, s4, s5, s6, s7)
            start = weight_copies(place_ref, plane, wall, sem_w, units)
            arrived = [start(0)]
        if n == 2:
            arrived.append(start(1))
        columns = slice(n * BAND, (n + 1) * BAND)
        total[RIM:, columns] += jnp.dot(p3[...], wo[:, columns], preferred_element_type=F32)
        kept = total[:, columns].astype(BF)
        stream[:, columns] = kept
        wide = kept.astype(F32)
        squares = squares + jnp.sum(wide * wide, axis=-1, keepdims=True)
    scale = lax.rsqrt(squares / width + epsilon)
    for n in range(bands):
        columns = slice(n * BAND, (n + 1) * BAND)
        xin[:, columns] = (
            stream[:, columns].astype(F32) * scale * gain_ref[:, columns]
        ).astype(BF)
    own_ref[...] = stream[pl.ds(pl.multiple_of(RIM + tp_index * share, 16), share), :]
    shares = []
    for k, dst in ((2, qa), (2, qb), (1, q1), (3, q3), (0, q0)):
        first = lax.rem(tp_index + k, 4) * share
        if dst is qb:
            first = first + share // 2
        shares.append((pl.multiple_of(first, 16), dst))

    def stored(n):
        columns = pl.ds(n * BAND, BAND)
        for first, dst in shares:
            source = part.at[pl.ds(first, dst.shape[0]), columns]
            go(copies_q, source, dst.at[:, columns], sem_q)

    ffn_blocks(xin, wall, hid, part, tg_ref, tv_ref, arrived, start, stored)
    for copy in copies_q:
        copy.wait()


def ffn(place, pieces, total, far_weights, weights, gain, tg, tv):
    rows, width = total.shape
    rows = rows - RIM
    inner = pieces[0].shape[1]
    units = tg.shape[1]
    share = rows // 4
    hbm = pl.BlockSpec(memory_space=pl.ANY)
    vmem = pl.BlockSpec(memory_space=pltpu.VMEM)
    shape = jax.ShapeDtypeStruct
    return pl.pallas_call(
        ffn_kernel,
        in_specs=[pl.BlockSpec(memory_space=pltpu.SMEM)] + [hbm] * 21 + [vmem] * 3,
        out_specs=[hbm] * 5 + [vmem],
        out_shape=[shape((share, width), BF)] * 3
        + [
            shape((share // 2, width), BF),
            shape((share // 2, width), BF),
            shape((share, width), BF),
        ],
        scratch_shapes=[
            pltpu.VMEM((rows, inner), BF),
            pltpu.VMEM((inner, width), BF),
            pltpu.VMEM((rows + RIM, width), F32),
            pltpu.VMEM((16, 2, 2, width // 64, 3 * units), BF),
            pltpu.VMEM((rows + RIM, width), BF),
            pltpu.VMEM((rows + RIM, width), BF),
            pltpu.VMEM((rows, units), BF),
            pltpu.VMEM((rows, width), BF),
            pltpu.SemaphoreType.DMA((4,)),
            pltpu.SemaphoreType.DMA((4,)),
            pltpu.SemaphoreType.DMA((96,)),
            pltpu.SemaphoreType.DMA((20,)),
        ],
        compiler_params=pltpu.CompilerParams(vmem_limit_bytes=60 * 1024 * 1024),
        name="ffn",
    )(place, *pieces, total, *far_weights, *weights, gain, tg, tv)


def by_units(gate, value):
    return [
        part[:, at : at + size]
        for at, size in unit_blocks(gate.shape[1])
        for part in (gate, value)
    ]


def on_device(
    mixer_value_projection,
    write_vectors_projected,
    read_vectors_projected,
    output_gate_projected,
    step_size_scores,
    position_decay_extra,
    step_size_bias,
    head_decay_logarithm,
    value_filter_taps,
    write_filter_taps,
    read_filter_taps,
    gated_group_norm_gain,
    mixer_output_weight,
    residual,
    feedforward_norm_gain,
    feedforward_gate_weight,
    feedforward_value_weight,
    gate_filter_taps,
    single_value_filter_taps,
    feedforward_down_weight,
):
    row_count, inner = mixer_value_projection.shape
    core = lax.axis_index("sp_2")
    tp_index = lax.axis_index("tp")

    rows = jnp.concatenate(
        by_units(feedforward_gate_weight, feedforward_value_weight)
        + [feedforward_down_weight.T],
        1,
    )
    part = rows.shape[0] // 2
    keep = jnp.where(core == 0, rows[:part], rows[part:])
    got = swapped(jnp.where(core == 0, rows[part:], rows[:part]))
    piece = jnp.concatenate([jnp.where(core == 0, keep, got), jnp.where(core == 0, got, keep)], 0)
    behind, ahead, far = short_ring(lambda a, by: turned(a, 0, by), piece)
    plane = halved_ring(
        lambda a, by: turned(a, 1, by),
        jnp.concatenate([piece, behind], 0),
        jnp.concatenate([ahead, far], 0),
    )
    plane = [a.reshape(-1, 2, part, a.shape[1]) for a in plane]
    weights = [*plane, *named_swaps(plane)]

    own_half = lax.dynamic_slice_in_dim(mixer_output_weight, core * (inner // 2), inner // 2, 0)
    out_ring = short_ring(lambda a, by: shifted(a, "tp", by, True), own_half)
    out_weights = [mixer_output_weight, *out_ring, *named_swaps(out_ring)]

    rim = jnp.concatenate(
        [
            a[row_count - RIM :]
            for a in (
                mixer_value_projection,
                write_vectors_projected,
                read_vectors_projected,
                residual,
            )
        ],
        1,
    )
    rim = shifted(rim, SP, 1)
    scaled, write, read, entering, cum, grow, packed = mixer_local(
        mixer_value_projection,
        write_vectors_projected.T,
        read_vectors_projected.T,
        rim,
        step_size_scores.T,
        position_decay_extra.T,
        step_size_bias[None],
        head_decay_logarithm[None],
        value_filter_taps,
        write_filter_taps,
        read_filter_taps,
    )
    y = mixer_inside(scaled, write, read, entering, cum)
    state = state_before(packed)
    top, low = mixer_finish(
        y, read, grow, output_gate_projected, state, gated_group_norm_gain[None]
    )
    ring = halved_ring(lambda a, by: shifted(a, "tp", by, True), top, low)
    near, far = ring[:6], ring[6:]
    halo = shifted(low[low.shape[0] - RIM :], SP, 1)
    halo = sent_to_all(halo, "tp")
    places = [lax.axis_index("sp_0"), lax.axis_index("sp_1"), core, tp_index]
    place = jnp.stack(places).astype(jnp.int32)
    total = out_near(place, near, halo, residual, rim, out_weights)
    far_weights = (out_weights[3], out_weights[6])
    here, on, back, far_on, far_back, own = ffn(
        place,
        far,
        total,
        far_weights,
        weights,
        feedforward_norm_gain[None],
        gate_filter_taps,
        single_value_filter_taps,
    )
    more_on = shifted(far_on, "tp", 1, True)
    more_back = shifted(far_back, "tp", -1, True)
    half = far_on.shape[0]
    on = (on.astype(F32) + jnp.pad(more_on.astype(F32), ((0, half), (0, 0)))).astype(BF)
    back = (back.astype(F32) + jnp.pad(more_back.astype(F32), ((half, 0), (0, 0)))).astype(BF)
    from_behind = shifted(on, "tp", 1, True)
    from_ahead = shifted(back, "tp", -1, True)
    down = here.astype(F32) + from_behind.astype(F32) + from_ahead.astype(F32)
    return (own.astype(F32) + down).astype(BF)


def solution(mesh):
    torus = Mesh(mesh.devices.reshape(4, 4, 2, mesh.shape["tp"]), ("sp_0", "sp_1", "sp_2", "tp"))
    in_specs = (
        P(SP, "tp"),
        P(SP, "tp"),
        P(SP, "tp"),
        P(SP, "tp"),
        P(SP, "tp"),
        P(SP, "tp"),
        P("tp"),
        P("tp"),
        P(None, "tp"),
        P(None, "tp"),
        P(None, "tp"),
        P("tp"),
        P("tp", None),
        P(SP, None),
        P(),
        P(SP, "tp"),
        P(SP, "tp"),
        P(None, "tp"),
        P(None, "tp"),
        P("tp", SP),
    )
    out_specs = P(SP_TP, None)

    return jax.shard_map(
        on_device, mesh=torus, in_specs=in_specs, out_specs=out_specs, check_vma=False
    )
```

```python
import jax
import jax.numpy as jnp
from jax import lax
from jax.experimental import pallas as pl
from jax.experimental.pallas import tpu as pltpu
from jax.sharding import Mesh
from jax.sharding import PartitionSpec as P


HEAD = 64
STATE = 64
BLOCK = 128
RIM = 16
SP = ("sp_0", "sp_1", "sp_2")
SP_TP = ("sp_0", "sp_1", "sp_2", "tp")
BF = jnp.bfloat16
F32 = jnp.float32

epsilon = 1e-06


def shifted(value, axis, by, wrap=False):
    length = lax.axis_size(axis)
    if wrap:
        pairs = [(i, (i + by) % length) for i in range(length)]
    else:
        pairs = [(i, i + by) for i in range(length) if 0 <= i + by < length]
    return lax.ppermute(value, axis, pairs)


def swapped(value):
    return lax.ppermute(value, "sp_2", [(0, 1), (1, 0)])


def turned(value, phase, by):
    zs, ys, cs = (lax.axis_size(axis) for axis in SP)
    pairs = []
    for z in range(zs):
        for y in range(ys):
            for c in range(cs):
                to_z, to_y = (z, (y + by) % ys) if c == phase else ((z + by) % zs, y)
                pairs.append(((z * ys + y) * cs + c, (to_z * ys + to_y) * cs + c))
    return lax.ppermute(value, SP, pairs)


def short_ring(step, value):
    behind = step(value, 1)
    ahead = step(value, -1)
    far = step(behind, 1)
    return behind, ahead, far


def named_swaps(values):
    result = []
    for value in values:
        result.append(swapped(value))
    return result


def sent_to_all(value, axis):
    length = lax.axis_size(axis)
    return lax.all_to_all(
        jnp.broadcast_to(value[None], (length, *value.shape)), axis, 0, 0, tiled=True
    )


def silu(v):
    return v / (1.0 + jnp.exp(-v))


def rolled_taps(before, current, taps):
    count = taps.shape[0]
    rows = current.shape[0]
    padded = jnp.concatenate([before, current], 0)
    result = taps[count - 1 : count].astype(F32) * current
    for back in range(1, count):
        moved = pltpu.roll(padded, back, 0)[8 : 8 + rows]
        result = result + taps[count - 1 - back : count - back].astype(F32) * moved
    return result


def halves(a, axis):
    high = a.astype(BF)
    return jnp.concatenate([high, (a - high.astype(F32)).astype(BF)], axis)


def thirds(a, axis):
    high = a.astype(BF)
    rest = a - high.astype(F32)
    middle = rest.astype(BF)
    return jnp.concatenate([high, middle, (rest - middle.astype(F32)).astype(BF)], axis)


def head_lanes(heads, inner):
    one = (
        lax.broadcasted_iota(jnp.int32, (heads, inner), 1) // HEAD
        == lax.broadcasted_iota(jnp.int32, (heads, inner), 0)
    ).astype(F32)
    return jnp.concatenate([one, one], 0).astype(BF)


def spread(by_head, lanes):
    return lax.dot_general(
        halves(by_head, 0), lanes, (((0,), (0,)), ((), ())), preferred_element_type=F32
    )


def mixer_kernel(
    x_ref, w_ref, r_ref, rim_ref, dt_ref, ex_ref, bias_ref, rate_ref,
    tx_ref, tw_ref, tr_ref,
    scaled_ref, write_ref, read_ref, before_ref, cum_ref, grow_ref, state_ref,
    carry, total, bx, bw, br,
):
    step_index = pl.program_id(0)
    heads = dt_ref.shape[0]
    size, inner = x_ref.shape

    @pl.when(step_index == 0)
    def _():
        carry[...] = jnp.zeros_like(carry)
        total[...] = jnp.zeros_like(total)
        rim = rim_ref[RIM - 8 :, : inner + 2 * STATE].astype(F32)
        bx[...] = rim[:, :inner]
        bw[...] = rim[:, inner : inner + STATE]
        br[...] = rim[:, inner + STATE :]

    cx = x_ref[...].astype(F32)
    cw = w_ref[...].astype(F32).T
    cr = r_ref[...].astype(F32).T
    x = silu(rolled_taps(bx[...], cx, tx_ref[...])).astype(BF)
    write = silu(rolled_taps(bw[...], cw, tw_ref[...])).astype(BF)
    read = silu(rolled_taps(br[...], cr, tr_ref[...])).astype(BF)
    bx[...] = cx[size - 8 :]
    bw[...] = cw[size - 8 :]
    br[...] = cr[size - 8 :]
    write_ref[...] = write
    read_ref[...] = read

    lanes = head_lanes(heads, inner)
    column = lambda a: jnp.broadcast_to(a, (heads, heads)).T[:, :1]
    raw = dt_ref[...] + column(bias_ref[...])
    step = jnp.maximum(raw, 0.0) + jnp.log1p(jnp.exp(-jnp.abs(raw)))
    log_decay = -step * jnp.exp(column(rate_ref[...])) + ex_ref[...]
    upper = (
        lax.broadcasted_iota(jnp.int32, (BLOCK, BLOCK), 0)
        <= lax.broadcasted_iota(jnp.int32, (BLOCK, BLOCK), 1)
    ).astype(F32).astype(BF)
    state = carry[...]
    sum_before = total[...]
    scaled = (x.astype(F32) * spread(step, lanes)).astype(BF)
    scaled_ref[...] = scaled
    for k in range(size // BLOCK):
        here = slice(k * BLOCK, (k + 1) * BLOCK)
        parts = jnp.dot(thirds(log_decay[:, here], 0), upper, preferred_element_type=F32)
        cum = parts[:heads] + parts[heads : 2 * heads] + parts[2 * heads :]
        end = cum[:, BLOCK - 1 :]
        cum_ref[:, here] = cum
        grow_ref[:, here] = jnp.exp(cum + sum_before[:, :1])
        before_ref[k * STATE : (k + 1) * STATE, :] = state
        tails = spread(jnp.exp(end - cum), lanes)
        tailed = (scaled[here].astype(F32) * tails).astype(BF)
        fresh = lax.dot_general(
            write[here], tailed, (((0,), (0,)), ((), ())), preferred_element_type=F32
        )
        decay = spread(jnp.broadcast_to(jnp.exp(end), (heads, BLOCK)), lanes)
        state = state * decay[:1] + fresh
        sum_before = sum_before + end
    carry[...] = state
    total[...] = sum_before

    @pl.when(step_index == pl.num_programs(0) - 1)
    def _():
        state_ref[:STATE, :] = state.astype(BF)
        decay = spread(jnp.exp(sum_before), lanes)
        state_ref[STATE:, :] = decay[:RIM].astype(BF)


def mixer_local(x, w, r, rim, dt, ex, bias, rate, tx, tw, tr):
    rows, inner = x.shape
    heads = dt.shape[0]
    size = 2 * BLOCK
    by_block = lambda width: pl.BlockSpec((size, width), lambda b: (b, 0))
    by_lanes = pl.BlockSpec((heads, size), lambda b: (0, b))
    by_channel = pl.BlockSpec((STATE, size), lambda b: (0, b))
    whole = lambda a: pl.BlockSpec(a.shape, lambda b: (0, 0))
    shape = jax.ShapeDtypeStruct
    blocks = rows // BLOCK
    return pl.pallas_call(
        mixer_kernel,
        grid=(rows // size,),
        in_specs=[by_block(inner), by_channel, by_channel, whole(rim), by_lanes, by_lanes]
        + [whole(a) for a in (bias, rate, tx, tw, tr)],
        out_specs=[
            by_block(inner),
            by_block(STATE),
            by_block(STATE),
            pl.BlockSpec((size // BLOCK * STATE, inner), lambda b: (b, 0)),
            by_lanes,
            by_lanes,
            pl.BlockSpec((STATE + RIM, inner), lambda b: (0, 0)),
        ],
        out_shape=[
            shape((rows, inner), BF),
            shape((rows, STATE), BF),
            shape((rows, STATE), BF),
            shape((blocks * STATE, inner), F32),
            shape((heads, rows), F32),
            shape((heads, rows), F32),
            shape((STATE + RIM, inner), BF),
        ],
        scratch_shapes=[
            pltpu.VMEM((STATE, inner), F32),
            pltpu.VMEM((heads, BLOCK), F32),
            pltpu.VMEM((8, inner), F32),
            pltpu.VMEM((8, STATE), F32),
            pltpu.VMEM((8, STATE), F32),
        ],
        name="mixer_local",
    )(x, w, r, rim, dt, ex, bias, rate, tx, tw, tr)


def entered(read, state):
    return jnp.dot(
        jnp.concatenate([read, read], 1), halves(state, 0), preferred_element_type=F32
    )


def inside_kernel(scaled_ref, write_ref, read_ref, before_ref, cum_ref, y_ref):
    heads = cum_ref.shape[0]
    size, inner = scaled_ref.shape
    lanes = head_lanes(heads, inner)
    rows = lax.broadcasted_iota(jnp.int32, (BLOCK, BLOCK), 0)
    cols = lax.broadcasted_iota(jnp.int32, (BLOCK, BLOCK), 1)
    causal = rows >= cols
    first_half = lax.broadcasted_iota(jnp.int32, (BLOCK, 2 * HEAD), 1) < HEAD
    for k in range(size // BLOCK):
        here = slice(k * BLOCK, (k + 1) * BLOCK)
        read = read_ref[here, :]
        scaled = scaled_ref[here, :]
        cum_t = cum_ref[:, here]
        cum = cum_t.T
        scores = lax.dot_general(
            read, write_ref[here, :], (((1,), (1,)), ((), ())), preferred_element_type=F32
        )
        pieces = []
        for pair in range(heads // 2):
            values = scaled[:, pair * 2 * HEAD : (pair + 1) * 2 * HEAD]
            both = []
            for h in (2 * pair, 2 * pair + 1):
                gap = cum[:, h : h + 1] - cum_t[h : h + 1, :]
                both.append((scores * jnp.exp(jnp.where(causal, gap, -1e30))).astype(BF))
            product = jnp.dot(jnp.concatenate(both, 0), values, preferred_element_type=F32)
            pieces.append(jnp.where(first_half, product[:BLOCK], product[BLOCK:]))
        before = before_ref[k * STATE : (k + 1) * STATE, :]
        grown = spread(jnp.exp(cum_t), lanes)
        y_ref[here, :] = jnp.concatenate(pieces, 1) + grown * entered(read, before)


def mixer_inside(scaled, write, read, before, cum):
    rows, inner = scaled.shape
    heads = cum.shape[0]
    size = 2 * BLOCK
    by_block = lambda width: pl.BlockSpec((size, width), lambda b: (b, 0))
    return pl.pallas_call(
        inside_kernel,
        grid=(rows // size,),
        in_specs=[
            by_block(inner),
            by_block(STATE),
            by_block(STATE),
            pl.BlockSpec((size // BLOCK * STATE, inner), lambda b: (b, 0)),
            pl.BlockSpec((heads, size), lambda b: (0, b)),
        ],
        out_specs=by_block(inner),
        out_shape=jax.ShapeDtypeStruct((rows, inner), F32),
        name="mixer_inside",
    )(scaled, write, read, before, cum)


def finish_kernel(y_ref, read_ref, grow_ref, gate_ref, state_ref, gain_ref, top_ref, low_ref):
    grown = spread(grow_ref[...], head_lanes(grow_ref.shape[0], y_ref.shape[1]))
    mixer = y_ref[...] + grown * entered(read_ref[...], state_ref[...])
    gated = mixer * silu(gate_ref[...].astype(F32))
    mean = jnp.mean(gated * gated, axis=-1, keepdims=True)
    normed = (gated * lax.rsqrt(mean + epsilon) * gain_ref[...]).astype(BF)

    @pl.when(pl.program_id(0) == 0)
    def _():
        top_ref[...] = normed

    @pl.when(pl.program_id(0) == 1)
    def _():
        low_ref[...] = normed


def mixer_finish(y, read, grow, gate, state, gain):
    rows, inner = y.shape
    heads = grow.shape[0]
    size = rows // 2
    by_block = lambda width: pl.BlockSpec((size, width), lambda b: (b, 0))
    whole = lambda a: pl.BlockSpec(a.shape, lambda b: (0, 0))
    return pl.pallas_call(
        finish_kernel,
        grid=(rows // size,),
        in_specs=[by_block(inner), by_block(STATE), pl.BlockSpec((heads, size), lambda b: (0, b))]
        + [by_block(inner), whole(state), whole(gain)],
        out_specs=[pl.BlockSpec((size, inner), lambda b: (0, 0))] * 2,
        out_shape=[jax.ShapeDtypeStruct((size, inner), BF)] * 2,
        name="mixer_finish",
    )(y, read, grow, gate, state, gain)


def split_state(packed):
    packed = packed.astype(F32)
    return packed[..., STATE : STATE + 1, :], packed[..., :STATE, :]


def joined(earlier, later):
    return earlier[0] * later[0], earlier[1] * later[0] + later[1]


def packed_state(pair):
    decay = jnp.broadcast_to(pair[0], (RIM, pair[0].shape[1]))
    return jnp.concatenate([pair[1], decay], 0).astype(BF)


def state_before(packed):
    own = split_state(packed)
    other = split_state(swapped(packed))
    late = lax.axis_index("sp_2") == 1
    first = jax.tree.map(lambda a, b: jnp.where(late, a, b), other, own)
    second = jax.tree.map(lambda a, b: jnp.where(late, a, b), own, other)
    running = joined(first, second)
    before = (
        jnp.where(late, other[0], 1.0),
        jnp.where(late, other[1], 0.0),
    )
    for axis in ("sp_1", "sp_0"):
        here = lax.axis_index(axis)
        all_of = sent_to_all(packed_state(running), axis)
        decay, state = split_state(all_of)
        whole = (jnp.ones_like(decay[0]), jnp.zeros_like(state[0]))
        inside = whole
        for k in range(lax.axis_size(axis)):
            whole = joined(whole, (decay[k], state[k]))
            passed = k < here
            inside = jax.tree.map(lambda new, old: jnp.where(passed, new, old), whole, inside)
        before = joined(inside, before)
        running = whole
    return before[1]


def halved_ring(step, top, low):
    result = {}
    for key, value, by in (
        ("bt", top, 1), ("al", low, -1), ("bl", low, 1), ("at", top, -1),
    ):
        result[key] = step(value, by)
    far_top = step(result["bt"], 1)
    far_low = step(result["al"], -1)
    return [
        top, low, result["bt"], result["bl"], result["at"], result["al"], far_top, far_low,
    ]


def rolled(rows, taps):
    count = taps.shape[0]
    result = taps[count - 1 : count] * rows
    for back in range(1, count):
        result = result + taps[count - 1 - back : count - back] * pltpu.roll(rows, back, 0)
    return result


HOPS = (0, -1, 1, 2)


BAND = 512


def go(into, src, dst, sems):
    copy = pltpu.make_async_copy(src, dst, sems.at[len(into)])
    copy.start()
    into.append(copy)


def near_kernel(
    place_ref, p0, l0, p1, l1, p2, l2, halo, res, rim, o0, ob, oa, of, tb, ta, tf,
    total_out,
    x, wo, stream, total, sem_x, sem_o, sem_t,
):
    core = place_ref[2]
    tp_index = place_ref[3]
    rows, width = res.shape
    inner = p0.shape[1]
    half = inner // 2
    near = 3 * inner
    copies_x, copies_o = [], []
    for k, by in enumerate(HOPS):
        at = lax.rem(tp_index + (by + 4), 4)
        columns = pl.ds(k * inner, inner)
        if k < 3:
            top, low = ((p0, l0), (p1, l1), (p2, l2))[k]
            go(copies_x, top, x.at[pl.ds(RIM, rows // 2), columns], sem_x)
            go(copies_x, low, x.at[pl.ds(RIM + rows // 2, rows // 2), columns], sem_x)
        go(copies_x, halo.at[at], x.at[pl.ds(0, RIM), columns], sem_x)
    bands = width // BAND

    def out_weight(n):
        columns = pl.ds(n * BAND, BAND)
        go(copies_o, o0.at[:, columns], wo.at[pl.ds(0, inner), columns], sem_o)
        for side, pieces in ((core, (ob, oa, of)), (1 - core, (tb, ta, tf))):
            first = pl.multiple_of(side * half, half)
            for k, src in enumerate(pieces):
                into = pl.ds((k + 1) * inner + first, half)
                go(copies_o, src.at[:, columns], wo.at[into, columns], sem_o)

    out_weight(0)
    go(copies_x, rim.at[:, pl.ds(rim.shape[1] - width, width)], stream.at[pl.ds(0, RIM)], sem_x)
    go(copies_x, res, stream.at[pl.ds(RIM, rows)], sem_x)
    for n in range(1, bands):
        out_weight(n)
    for copy in copies_x + copies_o:
        copy.wait()

    def store(n):
        columns = pl.ds(n * BAND, BAND)
        return pltpu.make_async_copy(total.at[:, columns], total_out.at[:, columns], sem_t.at[n])

    def band(n, _):
        columns = pl.ds(pl.multiple_of(n * BAND, BAND), BAND)
        total[:, columns] = stream[:, columns].astype(F32) + jnp.dot(
            x[:, :near], wo[:near, columns], preferred_element_type=F32
        )
        total[:RIM, columns] += jnp.dot(
            x[:RIM, near:], wo[near:, columns], preferred_element_type=F32
        )
        store(n).start()
        return 0

    lax.fori_loop(0, bands, band, 0)
    for n in range(bands):
        store(n).wait()


def out_near(place, pieces, halo, residual, rim, out_weights):
    rows, width = residual.shape
    hbm = pl.BlockSpec(memory_space=pl.ANY)
    return pl.pallas_call(
        near_kernel,
        in_specs=[pl.BlockSpec(memory_space=pltpu.SMEM)] + [hbm] * 16,
        out_specs=hbm,
        out_shape=jax.ShapeDtypeStruct((rows + RIM, width), F32),
        scratch_shapes=[
            pltpu.VMEM((rows + RIM, width), BF),
            pltpu.VMEM((width, width), BF),
            pltpu.VMEM((rows + RIM, width), BF),
            pltpu.VMEM((rows + RIM, width), F32),
            pltpu.SemaphoreType.DMA((12,)),
            pltpu.SemaphoreType.DMA((28,)),
            pltpu.SemaphoreType.DMA((4,)),
        ],
        compiler_params=pltpu.CompilerParams(vmem_limit_bytes=60 * 1024 * 1024),
        name="out_near",
    )(place, *pieces, halo, residual, rim, *out_weights)


UNIT = 256


def unit_blocks(units):
    return [(at, min(UNIT, units - at)) for at in range(0, units, UNIT)]


def weight_copies(place_ref, plane, wall, sems, units):
    z_index = place_ref[0]
    y_index = place_ref[1]
    core = place_ref[2]
    every = []
    stretches = ((0, 2 * UNIT), (2 * UNIT, 2 * units), (2 * units, 3 * units))

    def start(stretch):
        lanes = pl.ds(stretches[stretch][0], stretches[stretch][1] - stretches[stretch][0])
        done = len(every)
        for side, sources in ((core, plane[:8]), (1 - core, plane[8:])):
            first_axis = jnp.where(side == 0, y_index, z_index)
            second_axis = jnp.where(side == 0, z_index, y_index)
            for m, by_second in enumerate(HOPS):
                second = lax.rem(second_axis + (by_second + 4), 4)
                for k, by_first in enumerate((0, -1, 1, 2)):
                    first = lax.rem(first_axis + (by_first + 4), 4)
                    chip = jnp.where(side == 0, second * 4 + first, first * 4 + second)
                    src = sources[2 * m + k // 2].at[k % 2, :, :, lanes]
                    go(every, src, wall.at[chip, :, side, :, lanes], sems)
        return every[done:]

    return start


def ffn_blocks(xin, wall, hid, part, tg_ref, tv_ref, arrived, start, stored):
    width = xin.shape[1]
    units = hid.shape[1]
    for j, (at, size) in enumerate(unit_blocks(units)):
        if j < 2:
            for copy in arrived[j]:
                copy.wait()
        if j == 0:
            arrived.append(start(2))
        weight = wall[..., 2 * at : 2 * (at + size)].reshape(width, 2 * size)
        rows = jnp.dot(xin[...], weight, preferred_element_type=F32).astype(BF).astype(F32)
        taps = jnp.concatenate([tg_ref[:, at : at + size], tv_ref[:, at : at + size]], 1)
        rows = rolled(rows, taps.astype(F32))
        act = (silu(rows[:, :size]) * rows[:, size:]).astype(BF)
        hid[:, at : at + size] = act[RIM:]
    for copy in arrived[2]:
        copy.wait()
    bands = width // BAND
    chips = wall.shape[0] // bands

    def band(n, _):
        weight = wall[pl.ds(n * chips, chips), :, :, :, 2 * units :].reshape(BAND, units)
        part[:, pl.ds(pl.multiple_of(n * BAND, BAND), BAND)] = lax.dot_general(
            hid[...], weight, (((1,), (1,)), ((), ())), preferred_element_type=F32
        ).astype(BF)
        stored(n)
        return 0

    lax.fori_loop(0, bands, band, 0)


def ffn_kernel(
    place_ref, p3a, p3b, total_in, of, tf,
    w0, w1, w2, w3, w4, w5, w6, w7, s0, s1, s2, s3, s4, s5, s6, s7,
    gain_ref, tg_ref, tv_ref,
    q0, q1, q3, qa, qb, own_ref,
    p3, wo, total, wall, stream, xin, hid, part, sem_x, sem_t, sem_w, sem_q,
):
    core = place_ref[2]
    tp_index = place_ref[3]
    rows, inner = p3.shape
    width = wo.shape[1]
    units = hid.shape[1]
    half = inner // 2
    share = rows // 4
    bands = width // BAND
    copies_x, copies_t = [], []
    go(copies_x, p3a, p3.at[pl.ds(0, rows // 2)], sem_x)
    go(copies_x, p3b, p3.at[pl.ds(rows // 2, rows // 2)], sem_x)
    go(copies_x, of, wo.at[pl.ds(pl.multiple_of(core * half, half), half)], sem_x)
    go(copies_x, tf, wo.at[pl.ds(pl.multiple_of((1 - core) * half, half), half)], sem_x)
    for n in range(bands):
        columns = pl.ds(n * BAND, BAND)
        go(copies_t, total_in.at[:, columns], total.at[:, columns], sem_t)
    for copy in copies_x:
        copy.wait()
    squares = jnp.zeros((rows + RIM, 1), F32)
    for n in range(bands):
        copies_t[n].wait()
        if n == 1:
            plane = (w0, w1, w2, w3, w4, w5, w6, w7, s0, s1, s2, s3, s4, s5, s6, s7)
            start = weight_copies(place_ref, plane, wall, sem_w, units)
            arrived = [start(0)]
        if n == 2:
            arrived.append(start(1))
        columns = slice(n * BAND, (n + 1) * BAND)
        total[RIM:, columns] += jnp.dot(p3[...], wo[:, columns], preferred_element_type=F32)
        kept = total[:, columns].astype(BF)
        stream[:, columns] = kept
        wide = kept.astype(F32)
        squares = squares + jnp.sum(wide * wide, axis=-1, keepdims=True)
    scale = lax.rsqrt(squares / width + epsilon)
    for n in range(bands):
        columns = slice(n * BAND, (n + 1) * BAND)
        xin[:, columns] = (
            stream[:, columns].astype(F32) * scale * gain_ref[:, columns]
        ).astype(BF)
    own_ref[...] = stream[pl.ds(pl.multiple_of(RIM + tp_index * share, 16), share), :]
    shares = []
    for k, dst in ((2, qa), (2, qb), (1, q1), (3, q3), (0, q0)):
        first = lax.rem(tp_index + k, 4) * share
        if dst is qb:
            first = first + share // 2
        shares.append((pl.multiple_of(first, 16), dst))

    def stores(n):
        columns = pl.ds(n * BAND, BAND)
        return [
            pltpu.make_async_copy(
                part.at[pl.ds(first, dst.shape[0]), columns],
                dst.at[:, columns],
                sem_q.at[n * len(shares) + i],
            )
            for i, (first, dst) in enumerate(shares)
        ]

    def stored(n):
        for copy in stores(n):
            copy.start()

    ffn_blocks(xin, wall, hid, part, tg_ref, tv_ref, arrived, start, stored)
    for n in range(bands):
        for copy in stores(n):
            copy.wait()


def ffn(place, pieces, total, far_weights, weights, gain, tg, tv):
    rows, width = total.shape
    rows = rows - RIM
    inner = pieces[0].shape[1]
    units = tg.shape[1]
    share = rows // 4
    hbm = pl.BlockSpec(memory_space=pl.ANY)
    vmem = pl.BlockSpec(memory_space=pltpu.VMEM)
    shape = jax.ShapeDtypeStruct
    return pl.pallas_call(
        ffn_kernel,
        in_specs=[pl.BlockSpec(memory_space=pltpu.SMEM)] + [hbm] * 21 + [vmem] * 3,
        out_specs=[hbm] * 5 + [vmem],
        out_shape=[shape((share, width), BF)] * 3
        + [
            shape((share // 2, width), BF),
            shape((share // 2, width), BF),
            shape((share, width), BF),
        ],
        scratch_shapes=[
            pltpu.VMEM((rows, inner), BF),
            pltpu.VMEM((inner, width), BF),
            pltpu.VMEM((rows + RIM, width), F32),
            pltpu.VMEM((16, 2, 2, width // 64, 3 * units), BF),
            pltpu.VMEM((rows + RIM, width), BF),
            pltpu.VMEM((rows + RIM, width), BF),
            pltpu.VMEM((rows, units), BF),
            pltpu.VMEM((rows, width), BF),
            pltpu.SemaphoreType.DMA((4,)),
            pltpu.SemaphoreType.DMA((4,)),
            pltpu.SemaphoreType.DMA((96,)),
            pltpu.SemaphoreType.DMA((20,)),
        ],
        compiler_params=pltpu.CompilerParams(vmem_limit_bytes=60 * 1024 * 1024),
        name="ffn",
    )(place, *pieces, total, *far_weights, *weights, gain, tg, tv)


def by_units(gate, value):
    return [
        part[:, at : at + size]
        for at, size in unit_blocks(gate.shape[1])
        for part in (gate, value)
    ]


def on_device(
    mixer_value_projection,
    write_vectors_projected,
    read_vectors_projected,
    output_gate_projected,
    step_size_scores,
    position_decay_extra,
    step_size_bias,
    head_decay_logarithm,
    value_filter_taps,
    write_filter_taps,
    read_filter_taps,
    gated_group_norm_gain,
    mixer_output_weight,
    residual,
    feedforward_norm_gain,
    feedforward_gate_weight,
    feedforward_value_weight,
    gate_filter_taps,
    single_value_filter_taps,
    feedforward_down_weight,
):
    row_count, inner = mixer_value_projection.shape
    core = lax.axis_index("sp_2")
    tp_index = lax.axis_index("tp")

    rows = jnp.concatenate(
        by_units(feedforward_gate_weight, feedforward_value_weight)
        + [feedforward_down_weight.T],
        1,
    )
    part = rows.shape[0] // 2
    keep = jnp.where(core == 0, rows[:part], rows[part:])
    got = swapped(jnp.where(core == 0, rows[part:], rows[:part]))
    piece = jnp.concatenate([jnp.where(core == 0, keep, got), jnp.where(core == 0, got, keep)], 0)
    behind, ahead, far = short_ring(lambda a, by: turned(a, 0, by), piece)
    plane = halved_ring(
        lambda a, by: turned(a, 1, by),
        jnp.concatenate([piece, behind], 0),
        jnp.concatenate([ahead, far], 0),
    )
    plane = [a.reshape(-1, 2, part, a.shape[1]) for a in plane]
    weights = [*plane, *named_swaps(plane)]

    own_half = lax.dynamic_slice_in_dim(mixer_output_weight, core * (inner // 2), inner // 2, 0)
    out_ring = short_ring(lambda a, by: shifted(a, "tp", by, True), own_half)
    out_weights = [mixer_output_weight, *out_ring, *named_swaps(out_ring)]

    rim = jnp.concatenate(
        [
            a[row_count - RIM :]
            for a in (
                mixer_value_projection,
                write_vectors_projected,
                read_vectors_projected,
                residual,
            )
        ],
        1,
    )
    rim = shifted(rim, SP, 1)
    scaled, write, read, entering, cum, grow, packed = mixer_local(
        mixer_value_projection,
        write_vectors_projected.T,
        read_vectors_projected.T,
        rim,
        step_size_scores.T,
        position_decay_extra.T,
        step_size_bias[None],
        head_decay_logarithm[None],
        value_filter_taps,
        write_filter_taps,
        read_filter_taps,
    )
    y = mixer_inside(scaled, write, read, entering, cum)
    state = state_before(packed)
    top, low = mixer_finish(
        y, read, grow, output_gate_projected, state, gated_group_norm_gain[None]
    )
    ring = halved_ring(lambda a, by: shifted(a, "tp", by, True), top, low)
    near, far = ring[:6], ring[6:]
    halo = shifted(low[low.shape[0] - RIM :], SP, 1)
    halo = sent_to_all(halo, "tp")
    places = [lax.axis_index("sp_0"), lax.axis_index("sp_1"), core, tp_index]
    place = jnp.stack(places).astype(jnp.int32)
    total = out_near(place, near, halo, residual, rim, out_weights)
    far_weights = (out_weights[3], out_weights[6])
    here, on, back, far_on, far_back, own = ffn(
        place,
        far,
        total,
        far_weights,
        weights,
        feedforward_norm_gain[None],
        gate_filter_taps,
        single_value_filter_taps,
    )
    more_on = shifted(far_on, "tp", 1, True)
    more_back = shifted(far_back, "tp", -1, True)
    half = far_on.shape[0]
    on = (on.astype(F32) + jnp.pad(more_on.astype(F32), ((0, half), (0, 0)))).astype(BF)
    back = (back.astype(F32) + jnp.pad(more_back.astype(F32), ((half, 0), (0, 0)))).astype(BF)
    from_behind = shifted(on, "tp", 1, True)
    from_ahead = shifted(back, "tp", -1, True)
    down = here.astype(F32) + from_behind.astype(F32) + from_ahead.astype(F32)
    return (own.astype(F32) + down).astype(BF)


def solution(mesh):
    torus = Mesh(mesh.devices.reshape(4, 4, 2, mesh.shape["tp"]), ("sp_0", "sp_1", "sp_2", "tp"))
    in_specs = (
        P(SP, "tp"),
        P(SP, "tp"),
        P(SP, "tp"),
        P(SP, "tp"),
        P(SP, "tp"),
        P(SP, "tp"),
        P("tp"),
        P("tp"),
        P(None, "tp"),
        P(None, "tp"),
        P(None, "tp"),
        P("tp"),
        P("tp", None),
        P(SP, None),
        P(),
        P(SP, "tp"),
        P(SP, "tp"),
        P(None, "tp"),
        P(None, "tp"),
        P("tp", SP),
    )
    out_specs = P(SP_TP, None)

    return jax.shard_map(
        on_device, mesh=torus, in_specs=in_specs, out_specs=out_specs, check_vma=False
    )
```

```python
import jax
import jax.numpy as jnp
from jax import lax
from jax.experimental import pallas as pl
from jax.experimental.pallas import tpu as pltpu
from jax.sharding import Mesh
from jax.sharding import PartitionSpec as P


HEAD = 64
STATE = 64
BLOCK = 128
RIM = 16
SP = ("sp_0", "sp_1", "sp_2")
SP_TP = ("sp_0", "sp_1", "sp_2", "tp")
BF = jnp.bfloat16
F32 = jnp.float32

epsilon = 1e-06


def shifted(value, axis, by, wrap=False):
    length = lax.axis_size(axis)
    if wrap:
        pairs = [(i, (i + by) % length) for i in range(length)]
    else:
        pairs = [(i, i + by) for i in range(length) if 0 <= i + by < length]
    return lax.ppermute(value, axis, pairs)


def swapped(value):
    return lax.ppermute(value, "sp_2", [(0, 1), (1, 0)])


def turned(value, phase, by):
    zs, ys, cs = (lax.axis_size(axis) for axis in SP)
    pairs = []
    for z in range(zs):
        for y in range(ys):
            for c in range(cs):
                to_z, to_y = (z, (y + by) % ys) if c == phase else ((z + by) % zs, y)
                pairs.append(((z * ys + y) * cs + c, (to_z * ys + to_y) * cs + c))
    return lax.ppermute(value, SP, pairs)


def short_ring(step, value):
    behind = step(value, 1)
    ahead = step(value, -1)
    far = step(behind, 1)
    return behind, ahead, far


def named_swaps(values):
    result = []
    for value in values:
        result.append(swapped(value))
    return result


def sent_to_all(value, axis):
    length = lax.axis_size(axis)
    return lax.all_to_all(
        jnp.broadcast_to(value[None], (length, *value.shape)), axis, 0, 0, tiled=True
    )


def silu(v):
    return v / (1.0 + jnp.exp(-v))


def rolled_taps(before, current, taps):
    count = taps.shape[0]
    rows = current.shape[0]
    padded = jnp.concatenate([before, current], 0)
    result = taps[count - 1 : count].astype(F32) * current
    for back in range(1, count):
        moved = pltpu.roll(padded, back, 0)[8 : 8 + rows]
        result = result + taps[count - 1 - back : count - back].astype(F32) * moved
    return result


def halves(a, axis):
    high = a.astype(BF)
    return jnp.concatenate([high, (a - high.astype(F32)).astype(BF)], axis)


def thirds(a, axis):
    high = a.astype(BF)
    rest = a - high.astype(F32)
    middle = rest.astype(BF)
    return jnp.concatenate([high, middle, (rest - middle.astype(F32)).astype(BF)], axis)


def head_lanes(heads, inner):
    one = (
        lax.broadcasted_iota(jnp.int32, (heads, inner), 1) // HEAD
        == lax.broadcasted_iota(jnp.int32, (heads, inner), 0)
    ).astype(F32)
    return jnp.concatenate([one, one], 0).astype(BF)


def spread(by_head, lanes):
    return lax.dot_general(
        halves(by_head, 0), lanes, (((0,), (0,)), ((), ())), preferred_element_type=F32
    )


def mixer_kernel(
    x_ref, w_ref, r_ref, rim_ref, dt_ref, ex_ref, bias_ref, rate_ref,
    tx_ref, tw_ref, tr_ref,
    scaled_ref, write_ref, read_ref, before_ref, cum_ref, grow_ref, state_ref,
    carry, total, bx, bw, br,
):
    step_index = pl.program_id(0)
    heads = dt_ref.shape[0]
    size, inner = x_ref.shape

    @pl.when(step_index == 0)
    def _():
        carry[...] = jnp.zeros_like(carry)
        total[...] = jnp.zeros_like(total)
        rim = rim_ref[RIM - 8 :, : inner + 2 * STATE].astype(F32)
        bx[...] = rim[:, :inner]
        bw[...] = rim[:, inner : inner + STATE]
        br[...] = rim[:, inner + STATE :]

    cx = x_ref[...].astype(F32)
    cw = w_ref[...].astype(F32).T
    cr = r_ref[...].astype(F32).T
    x = silu(rolled_taps(bx[...], cx, tx_ref[...])).astype(BF)
    write = silu(rolled_taps(bw[...], cw, tw_ref[...])).astype(BF)
    read = silu(rolled_taps(br[...], cr, tr_ref[...])).astype(BF)
    bx[...] = cx[size - 8 :]
    bw[...] = cw[size - 8 :]
    br[...] = cr[size - 8 :]
    write_ref[...] = write
    read_ref[...] = read

    lanes = head_lanes(heads, inner)
    column = lambda a: jnp.broadcast_to(a, (heads, heads)).T[:, :1]
    raw = dt_ref[...] + column(bias_ref[...])
    step = jnp.maximum(raw, 0.0) + jnp.log1p(jnp.exp(-jnp.abs(raw)))
    log_decay = -step * jnp.exp(column(rate_ref[...])) + ex_ref[...]
    upper = (
        lax.broadcasted_iota(jnp.int32, (BLOCK, BLOCK), 0)
        <= lax.broadcasted_iota(jnp.int32, (BLOCK, BLOCK), 1)
    ).astype(F32).astype(BF)
    state = carry[...]
    sum_before = total[...]
    scaled = (x.astype(F32) * spread(step, lanes)).astype(BF)
    scaled_ref[...] = scaled
    for k in range(size // BLOCK):
        here = slice(k * BLOCK, (k + 1) * BLOCK)
        parts = jnp.dot(thirds(log_decay[:, here], 0), upper, preferred_element_type=F32)
        cum = parts[:heads] + parts[heads : 2 * heads] + parts[2 * heads :]
        end = cum[:, BLOCK - 1 :]
        cum_ref[:, here] = cum
        grow_ref[:, here] = jnp.exp(cum + sum_before[:, :1])
        before_ref[k * STATE : (k + 1) * STATE, :] = state
        tails = spread(jnp.exp(end - cum), lanes)
        tailed = (scaled[here].astype(F32) * tails).astype(BF)
        fresh = lax.dot_general(
            write[here], tailed, (((0,), (0,)), ((), ())), preferred_element_type=F32
        )
        decay = spread(jnp.broadcast_to(jnp.exp(end), (heads, BLOCK)), lanes)
        state = state * decay[:1] + fresh
        sum_before = sum_before + end
    carry[...] = state
    total[...] = sum_before

    @pl.when(step_index == pl.num_programs(0) - 1)
    def _():
        state_ref[:STATE, :] = state.astype(BF)
        decay = spread(jnp.exp(sum_before), lanes)
        state_ref[STATE:, :] = decay[:RIM].astype(BF)


def mixer_local(x, w, r, rim, dt, ex, bias, rate, tx, tw, tr):
    rows, inner = x.shape
    heads = dt.shape[0]
    size = 2 * BLOCK
    by_block = lambda width: pl.BlockSpec((size, width), lambda b: (b, 0))
    by_lanes = pl.BlockSpec((heads, size), lambda b: (0, b))
    by_channel = pl.BlockSpec((STATE, size), lambda b: (0, b))
    whole = lambda a: pl.BlockSpec(a.shape, lambda b: (0, 0))
    shape = jax.ShapeDtypeStruct
    blocks = rows // BLOCK
    return pl.pallas_call(
        mixer_kernel,
        grid=(rows // size,),
        in_specs=[by_block(inner), by_channel, by_channel, whole(rim), by_lanes, by_lanes]
        + [whole(a) for a in (bias, rate, tx, tw, tr)],
        out_specs=[
            by_block(inner),
            by_block(STATE),
            by_block(STATE),
            pl.BlockSpec((size // BLOCK * STATE, inner), lambda b: (b, 0)),
            by_lanes,
            by_lanes,
            pl.BlockSpec((STATE + RIM, inner), lambda b: (0, 0)),
        ],
        out_shape=[
            shape((rows, inner), BF),
            shape((rows, STATE), BF),
            shape((rows, STATE), BF),
            shape((blocks * STATE, inner), F32),
            shape((heads, rows), F32),
            shape((heads, rows), F32),
            shape((STATE + RIM, inner), BF),
        ],
        scratch_shapes=[
            pltpu.VMEM((STATE, inner), F32),
            pltpu.VMEM((heads, BLOCK), F32),
            pltpu.VMEM((8, inner), F32),
            pltpu.VMEM((8, STATE), F32),
            pltpu.VMEM((8, STATE), F32),
        ],
        name="mixer_local",
    )(x, w, r, rim, dt, ex, bias, rate, tx, tw, tr)


def entered(read, state):
    return jnp.dot(
        jnp.concatenate([read, read], 1), halves(state, 0), preferred_element_type=F32
    )


def inside_kernel(scaled_ref, write_ref, read_ref, before_ref, cum_ref, y_ref):
    heads = cum_ref.shape[0]
    size, inner = scaled_ref.shape
    lanes = head_lanes(heads, inner)
    rows = lax.broadcasted_iota(jnp.int32, (BLOCK, BLOCK), 0)
    cols = lax.broadcasted_iota(jnp.int32, (BLOCK, BLOCK), 1)
    causal = rows >= cols
    first_half = lax.broadcasted_iota(jnp.int32, (BLOCK, 2 * HEAD), 1) < HEAD
    for k in range(size // BLOCK):
        here = slice(k * BLOCK, (k + 1) * BLOCK)
        read = read_ref[here, :]
        scaled = scaled_ref[here, :]
        cum_t = cum_ref[:, here]
        cum = cum_t.T
        scores = lax.dot_general(
            read, write_ref[here, :], (((1,), (1,)), ((), ())), preferred_element_type=F32
        )
        pieces = []
        for pair in range(heads // 2):
            values = scaled[:, pair * 2 * HEAD : (pair + 1) * 2 * HEAD]
            both = []
            for h in (2 * pair, 2 * pair + 1):
                gap = cum[:, h : h + 1] - cum_t[h : h + 1, :]
                both.append((scores * jnp.exp(jnp.where(causal, gap, -1e30))).astype(BF))
            product = jnp.dot(jnp.concatenate(both, 0), values, preferred_element_type=F32)
            pieces.append(jnp.where(first_half, product[:BLOCK], product[BLOCK:]))
        before = before_ref[k * STATE : (k + 1) * STATE, :]
        grown = spread(jnp.exp(cum_t), lanes)
        y_ref[here, :] = jnp.concatenate(pieces, 1) + grown * entered(read, before)


def mixer_inside(scaled, write, read, before, cum):
    rows, inner = scaled.shape
    heads = cum.shape[0]
    size = 2 * BLOCK
    by_block = lambda width: pl.BlockSpec((size, width), lambda b: (b, 0))
    return pl.pallas_call(
        inside_kernel,
        grid=(rows // size,),
        in_specs=[
            by_block(inner),
            by_block(STATE),
            by_block(STATE),
            pl.BlockSpec((size // BLOCK * STATE, inner), lambda b: (b, 0)),
            pl.BlockSpec((heads, size), lambda b: (0, b)),
        ],
        out_specs=by_block(inner),
        out_shape=jax.ShapeDtypeStruct((rows, inner), F32),
        name="mixer_inside",
    )(scaled, write, read, before, cum)


def finish_kernel(y_ref, read_ref, grow_ref, gate_ref, state_ref, gain_ref, top_ref, low_ref):
    grown = spread(grow_ref[...], head_lanes(grow_ref.shape[0], y_ref.shape[1]))
    mixer = y_ref[...] + grown * entered(read_ref[...], state_ref[...])
    gated = mixer * silu(gate_ref[...].astype(F32))
    mean = jnp.mean(gated * gated, axis=-1, keepdims=True)
    normed = (gated * lax.rsqrt(mean + epsilon) * gain_ref[...]).astype(BF)

    @pl.when(pl.program_id(0) == 0)
    def _():
        top_ref[...] = normed

    @pl.when(pl.program_id(0) == 1)
    def _():
        low_ref[...] = normed


def mixer_finish(y, read, grow, gate, state, gain):
    rows, inner = y.shape
    heads = grow.shape[0]
    size = rows // 2
    by_block = lambda width: pl.BlockSpec((size, width), lambda b: (b, 0))
    whole = lambda a: pl.BlockSpec(a.shape, lambda b: (0, 0))
    return pl.pallas_call(
        finish_kernel,
        grid=(rows // size,),
        in_specs=[by_block(inner), by_block(STATE), pl.BlockSpec((heads, size), lambda b: (0, b))]
        + [by_block(inner), whole(state), whole(gain)],
        out_specs=[pl.BlockSpec((size, inner), lambda b: (0, 0))] * 2,
        out_shape=[jax.ShapeDtypeStruct((size, inner), BF)] * 2,
        name="mixer_finish",
    )(y, read, grow, gate, state, gain)


def split_state(packed):
    packed = packed.astype(F32)
    return packed[..., STATE : STATE + 1, :], packed[..., :STATE, :]


def joined(earlier, later):
    return earlier[0] * later[0], earlier[1] * later[0] + later[1]


def packed_state(pair):
    decay = jnp.broadcast_to(pair[0], (RIM, pair[0].shape[1]))
    return jnp.concatenate([pair[1], decay], 0).astype(BF)


def state_before(packed):
    own = split_state(packed)
    other = split_state(swapped(packed))
    late = lax.axis_index("sp_2") == 1
    first = jax.tree.map(lambda a, b: jnp.where(late, a, b), other, own)
    second = jax.tree.map(lambda a, b: jnp.where(late, a, b), own, other)
    running = joined(first, second)
    before = (
        jnp.where(late, other[0], 1.0),
        jnp.where(late, other[1], 0.0),
    )
    for axis in ("sp_1", "sp_0"):
        here = lax.axis_index(axis)
        all_of = sent_to_all(packed_state(running), axis)
        decay, state = split_state(all_of)
        whole = (jnp.ones_like(decay[0]), jnp.zeros_like(state[0]))
        inside = whole
        for k in range(lax.axis_size(axis)):
            whole = joined(whole, (decay[k], state[k]))
            passed = k < here
            inside = jax.tree.map(lambda new, old: jnp.where(passed, new, old), whole, inside)
        before = joined(inside, before)
        running = whole
    return before[1]


def halved_ring(step, top, low):
    result = {}
    for key, value, by in (
        ("bt", top, 1), ("al", low, -1), ("bl", low, 1), ("at", top, -1),
    ):
        result[key] = step(value, by)
    far_top = step(result["bt"], 1)
    far_low = step(result["al"], -1)
    return [
        top, low, result["bt"], result["bl"], result["at"], result["al"], far_top, far_low,
    ]


def rolled(rows, taps):
    count = taps.shape[0]
    result = taps[count - 1 : count] * rows
    for back in range(1, count):
        result = result + taps[count - 1 - back : count - back] * pltpu.roll(rows, back, 0)
    return result


HOPS = (0, -1, 1, 2)


BAND = 512


def go(into, src, dst, sems):
    copy = pltpu.make_async_copy(src, dst, sems.at[len(into)])
    copy.start()
    into.append(copy)


def near_kernel(
    place_ref, p0, l0, p1, l1, p2, l2, halo, res, rim, o0, ob, oa, of, tb, ta, tf,
    total_out,
    x, wo, stream, total, sem_x, sem_o, sem_t,
):
    core = place_ref[2]
    tp_index = place_ref[3]
    rows, width = res.shape
    inner = p0.shape[1]
    half = inner // 2
    near = 3 * inner
    copies_x, copies_o = [], []
    for k, by in enumerate(HOPS):
        at = lax.rem(tp_index + (by + 4), 4)
        columns = pl.ds(k * inner, inner)
        if k < 3:
            top, low = ((p0, l0), (p1, l1), (p2, l2))[k]
            go(copies_x, top, x.at[pl.ds(RIM, rows // 2), columns], sem_x)
            go(copies_x, low, x.at[pl.ds(RIM + rows // 2, rows // 2), columns], sem_x)
        go(copies_x, halo.at[at], x.at[pl.ds(0, RIM), columns], sem_x)
    bands = width // BAND

    def out_weight(n):
        columns = pl.ds(n * BAND, BAND)
        go(copies_o, o0.at[:, columns], wo.at[pl.ds(0, inner), columns], sem_o)
        for side, pieces in ((core, (ob, oa, of)), (1 - core, (tb, ta, tf))):
            first = pl.multiple_of(side * half, half)
            for k, src in enumerate(pieces):
                into = pl.ds((k + 1) * inner + first, half)
                go(copies_o, src.at[:, columns], wo.at[into, columns], sem_o)

    out_weight(0)
    go(copies_x, rim.at[:, pl.ds(rim.shape[1] - width, width)], stream.at[pl.ds(0, RIM)], sem_x)
    go(copies_x, res, stream.at[pl.ds(RIM, rows)], sem_x)
    for n in range(1, bands):
        out_weight(n)
    for copy in copies_x + copies_o[:7]:
        copy.wait()

    def store(n):
        columns = pl.ds(n * BAND, BAND)
        return pltpu.make_async_copy(total.at[:, columns], total_out.at[:, columns], sem_t.at[n])

    def band(n, _):
        columns = pl.ds(n * BAND if isinstance(n, int) else pl.multiple_of(n * BAND, BAND), BAND)
        total[:, columns] = stream[:, columns].astype(F32) + jnp.dot(
            x[:, :near], wo[:near, columns], preferred_element_type=F32
        )
        total[:RIM, columns] += jnp.dot(
            x[:RIM, near:], wo[near:, columns], preferred_element_type=F32
        )
        store(n).start()
        return 0

    band(0, 0)
    for copy in copies_o[7:]:
        copy.wait()
    lax.fori_loop(1, bands, band, 0)
    for n in range(bands):
        store(n).wait()


def out_near(place, pieces, halo, residual, rim, out_weights):
    rows, width = residual.shape
    hbm = pl.BlockSpec(memory_space=pl.ANY)
    return pl.pallas_call(
        near_kernel,
        in_specs=[pl.BlockSpec(memory_space=pltpu.SMEM)] + [hbm] * 16,
        out_specs=hbm,
        out_shape=jax.ShapeDtypeStruct((rows + RIM, width), F32),
        scratch_shapes=[
            pltpu.VMEM((rows + RIM, width), BF),
            pltpu.VMEM((width, width), BF),
            pltpu.VMEM((rows + RIM, width), BF),
            pltpu.VMEM((rows + RIM, width), F32),
            pltpu.SemaphoreType.DMA((12,)),
            pltpu.SemaphoreType.DMA((28,)),
            pltpu.SemaphoreType.DMA((4,)),
        ],
        compiler_params=pltpu.CompilerParams(vmem_limit_bytes=60 * 1024 * 1024),
        name="out_near",
    )(place, *pieces, halo, residual, rim, *out_weights)


UNIT = 256


def unit_blocks(units):
    return [(at, min(UNIT, units - at)) for at in range(0, units, UNIT)]


def weight_copies(place_ref, plane, wall, sems, units):
    z_index = place_ref[0]
    y_index = place_ref[1]
    core = place_ref[2]
    every = []
    stretches = ((0, 2 * UNIT), (2 * UNIT, 2 * units), (2 * units, 3 * units))

    def start(stretch):
        lanes = pl.ds(stretches[stretch][0], stretches[stretch][1] - stretches[stretch][0])
        done = len(every)
        for side, sources in ((core, plane[:8]), (1 - core, plane[8:])):
            first_axis = jnp.where(side == 0, y_index, z_index)
            second_axis = jnp.where(side == 0, z_index, y_index)
            for m, by_second in enumerate(HOPS):
                second = lax.rem(second_axis + (by_second + 4), 4)
                for k, by_first in enumerate((0, -1, 1, 2)):
                    first = lax.rem(first_axis + (by_first + 4), 4)
                    chip = jnp.where(side == 0, second * 4 + first, first * 4 + second)
                    src = sources[2 * m + k // 2].at[k % 2, :, :, lanes]
                    go(every, src, wall.at[chip, :, side, :, lanes], sems)
        return every[done:]

    return start


def ffn_blocks(xin, wall, hid, part, tg_ref, tv_ref, arrived, start, stored):
    width = xin.shape[1]
    units = hid.shape[1]
    for j, (at, size) in enumerate(unit_blocks(units)):
        if j < 2:
            for copy in arrived[j]:
                copy.wait()
        if j == 0:
            arrived.append(start(2))
        weight = wall[..., 2 * at : 2 * (at + size)].reshape(width, 2 * size)
        rows = jnp.dot(xin[...], weight, preferred_element_type=F32).astype(BF).astype(F32)
        taps = jnp.concatenate([tg_ref[:, at : at + size], tv_ref[:, at : at + size]], 1)
        rows = rolled(rows, taps.astype(F32))
        act = (silu(rows[:, :size]) * rows[:, size:]).astype(BF)
        hid[:, at : at + size] = act[RIM:]
    for copy in arrived[2]:
        copy.wait()
    bands = width // BAND
    chips = wall.shape[0] // bands

    def band(n, _):
        weight = wall[pl.ds(n * chips, chips), :, :, :, 2 * units :].reshape(BAND, units)
        part[:, pl.ds(pl.multiple_of(n * BAND, BAND), BAND)] = lax.dot_general(
            hid[...], weight, (((1,), (1,)), ((), ())), preferred_element_type=F32
        ).astype(BF)
        stored(n)
        return 0

    lax.fori_loop(0, bands, band, 0)


def ffn_kernel(
    place_ref, p3a, p3b, total_in, of, tf,
    w0, w1, w2, w3, w4, w5, w6, w7, s0, s1, s2, s3, s4, s5, s6, s7,
    gain_ref, tg_ref, tv_ref,
    q0, q1, q3, qa, qb, own_ref,
    p3, wo, total, wall, stream, xin, hid, part, sem_x, sem_t, sem_w, sem_q,
):
    core = place_ref[2]
    tp_index = place_ref[3]
    rows, inner = p3.shape
    width = wo.shape[1]
    units = hid.shape[1]
    half = inner // 2
    share = rows // 4
    bands = width // BAND
    copies_x, copies_t = [], []
    go(copies_x, p3a, p3.at[pl.ds(0, rows // 2)], sem_x)
    go(copies_x, p3b, p3.at[pl.ds(rows // 2, rows // 2)], sem_x)
    go(copies_x, of, wo.at[pl.ds(pl.multiple_of(core * half, half), half)], sem_x)
    go(copies_x, tf, wo.at[pl.ds(pl.multiple_of((1 - core) * half, half), half)], sem_x)
    for n in range(bands):
        columns = pl.ds(n * BAND, BAND)
        go(copies_t, total_in.at[:, columns], total.at[:, columns], sem_t)
    for copy in copies_x:
        copy.wait()
    squares = jnp.zeros((rows + RIM, 1), F32)
    for n in range(bands):
        copies_t[n].wait()
        if n == 1:
            plane = (w0, w1, w2, w3, w4, w5, w6, w7, s0, s1, s2, s3, s4, s5, s6, s7)
            start = weight_copies(place_ref, plane, wall, sem_w, units)
            arrived = [start(0)]
        if n == 2:
            arrived.append(start(1))
        columns = slice(n * BAND, (n + 1) * BAND)
        total[RIM:, columns] += jnp.dot(p3[...], wo[:, columns], preferred_element_type=F32)
        kept = total[:, columns].astype(BF)
        stream[:, columns] = kept
        wide = kept.astype(F32)
        squares = squares + jnp.sum(wide * wide, axis=-1, keepdims=True)
    scale = lax.rsqrt(squares / width + epsilon)
    for n in range(bands):
        columns = slice(n * BAND, (n + 1) * BAND)
        xin[:, columns] = (
            stream[:, columns].astype(F32) * scale * gain_ref[:, columns]
        ).astype(BF)
    own_ref[...] = stream[pl.ds(pl.multiple_of(RIM + tp_index * share, 16), share), :]
    shares = []
    for k, dst in ((2, qa), (2, qb), (1, q1), (3, q3), (0, q0)):
        first = lax.rem(tp_index + k, 4) * share
        if dst is qb:
            first = first + share // 2
        shares.append((pl.multiple_of(first, 16), dst))

    def stores(n):
        columns = pl.ds(n * BAND, BAND)
        return [
            pltpu.make_async_copy(
                part.at[pl.ds(first, dst.shape[0]), columns],
                dst.at[:, columns],
                sem_q.at[n * len(shares) + i],
            )
            for i, (first, dst) in enumerate(shares)
        ]

    def stored(n):
        for copy in stores(n):
            copy.start()

    ffn_blocks(xin, wall, hid, part, tg_ref, tv_ref, arrived, start, stored)
    for n in range(bands):
        for copy in stores(n):
            copy.wait()


def ffn(place, pieces, total, far_weights, weights, gain, tg, tv):
    rows, width = total.shape
    rows = rows - RIM
    inner = pieces[0].shape[1]
    units = tg.shape[1]
    share = rows // 4
    hbm = pl.BlockSpec(memory_space=pl.ANY)
    vmem = pl.BlockSpec(memory_space=pltpu.VMEM)
    shape = jax.ShapeDtypeStruct
    return pl.pallas_call(
        ffn_kernel,
        in_specs=[pl.BlockSpec(memory_space=pltpu.SMEM)] + [hbm] * 21 + [vmem] * 3,
        out_specs=[hbm] * 5 + [vmem],
        out_shape=[shape((share, width), BF)] * 3
        + [
            shape((share // 2, width), BF),
            shape((share // 2, width), BF),
            shape((share, width), BF),
        ],
        scratch_shapes=[
            pltpu.VMEM((rows, inner), BF),
            pltpu.VMEM((inner, width), BF),
            pltpu.VMEM((rows + RIM, width), F32),
            pltpu.VMEM((16, 2, 2, width // 64, 3 * units), BF),
            pltpu.VMEM((rows + RIM, width), BF),
            pltpu.VMEM((rows + RIM, width), BF),
            pltpu.VMEM((rows, units), BF),
            pltpu.VMEM((rows, width), BF),
            pltpu.SemaphoreType.DMA((4,)),
            pltpu.SemaphoreType.DMA((4,)),
            pltpu.SemaphoreType.DMA((96,)),
            pltpu.SemaphoreType.DMA((20,)),
        ],
        compiler_params=pltpu.CompilerParams(vmem_limit_bytes=60 * 1024 * 1024),
        name="ffn",
    )(place, *pieces, total, *far_weights, *weights, gain, tg, tv)


def by_units(gate, value):
    return [
        part[:, at : at + size]
        for at, size in unit_blocks(gate.shape[1])
        for part in (gate, value)
    ]


def on_device(
    mixer_value_projection,
    write_vectors_projected,
    read_vectors_projected,
    output_gate_projected,
    step_size_scores,
    position_decay_extra,
    step_size_bias,
    head_decay_logarithm,
    value_filter_taps,
    write_filter_taps,
    read_filter_taps,
    gated_group_norm_gain,
    mixer_output_weight,
    residual,
    feedforward_norm_gain,
    feedforward_gate_weight,
    feedforward_value_weight,
    gate_filter_taps,
    single_value_filter_taps,
    feedforward_down_weight,
):
    row_count, inner = mixer_value_projection.shape
    core = lax.axis_index("sp_2")
    tp_index = lax.axis_index("tp")

    rows = jnp.concatenate(
        by_units(feedforward_gate_weight, feedforward_value_weight)
        + [feedforward_down_weight.T],
        1,
    )
    part = rows.shape[0] // 2
    keep = jnp.where(core == 0, rows[:part], rows[part:])
    got = swapped(jnp.where(core == 0, rows[part:], rows[:part]))
    piece = jnp.concatenate([jnp.where(core == 0, keep, got), jnp.where(core == 0, got, keep)], 0)
    behind, ahead, far = short_ring(lambda a, by: turned(a, 0, by), piece)
    plane = halved_ring(
        lambda a, by: turned(a, 1, by),
        jnp.concatenate([piece, behind], 0),
        jnp.concatenate([ahead, far], 0),
    )
    plane = [a.reshape(-1, 2, part, a.shape[1]) for a in plane]
    weights = [*plane, *named_swaps(plane)]

    own_half = lax.dynamic_slice_in_dim(mixer_output_weight, core * (inner // 2), inner // 2, 0)
    out_ring = short_ring(lambda a, by: shifted(a, "tp", by, True), own_half)
    out_weights = [mixer_output_weight, *out_ring, *named_swaps(out_ring)]

    rim = jnp.concatenate(
        [
            a[row_count - RIM :]
            for a in (
                mixer_value_projection,
                write_vectors_projected,
                read_vectors_projected,
                residual,
            )
        ],
        1,
    )
    rim = shifted(rim, SP, 1)
    scaled, write, read, entering, cum, grow, packed = mixer_local(
        mixer_value_projection,
        write_vectors_projected.T,
        read_vectors_projected.T,
        rim,
        step_size_scores.T,
        position_decay_extra.T,
        step_size_bias[None],
        head_decay_logarithm[None],
        value_filter_taps,
        write_filter_taps,
        read_filter_taps,
    )
    y = mixer_inside(scaled, write, read, entering, cum)
    state = state_before(packed)
    top, low = mixer_finish(
        y, read, grow, output_gate_projected, state, gated_group_norm_gain[None]
    )
    ring = halved_ring(lambda a, by: shifted(a, "tp", by, True), top, low)
    near, far = ring[:6], ring[6:]
    halo = shifted(low[low.shape[0] - RIM :], SP, 1)
    halo = sent_to_all(halo, "tp")
    places = [lax.axis_index("sp_0"), lax.axis_index("sp_1"), core, tp_index]
    place = jnp.stack(places).astype(jnp.int32)
    total = out_near(place, near, halo, residual, rim, out_weights)
    far_weights = (out_weights[3], out_weights[6])
    here, on, back, far_on, far_back, own = ffn(
        place,
        far,
        total,
        far_weights,
        weights,
        feedforward_norm_gain[None],
        gate_filter_taps,
        single_value_filter_taps,
    )
    more_on = shifted(far_on, "tp", 1, True)
    more_back = shifted(far_back, "tp", -1, True)
    half = far_on.shape[0]
    on = (on.astype(F32) + jnp.pad(more_on.astype(F32), ((0, half), (0, 0)))).astype(BF)
    back = (back.astype(F32) + jnp.pad(more_back.astype(F32), ((half, 0), (0, 0)))).astype(BF)
    from_behind = shifted(on, "tp", 1, True)
    from_ahead = shifted(back, "tp", -1, True)
    down = here.astype(F32) + from_behind.astype(F32) + from_ahead.astype(F32)
    return (own.astype(F32) + down).astype(BF)


def solution(mesh):
    torus = Mesh(mesh.devices.reshape(4, 4, 2, mesh.shape["tp"]), ("sp_0", "sp_1", "sp_2", "tp"))
    in_specs = (
        P(SP, "tp"),
        P(SP, "tp"),
        P(SP, "tp"),
        P(SP, "tp"),
        P(SP, "tp"),
        P(SP, "tp"),
        P("tp"),
        P("tp"),
        P(None, "tp"),
        P(None, "tp"),
        P(None, "tp"),
        P("tp"),
        P("tp", None),
        P(SP, None),
        P(),
        P(SP, "tp"),
        P(SP, "tp"),
        P(None, "tp"),
        P(None, "tp"),
        P("tp", SP),
    )
    out_specs = P(SP_TP, None)

    return jax.shard_map(
        on_device, mesh=torus, in_specs=in_specs, out_specs=out_specs, check_vma=False
    )
```
